32 devices in a mesh: sp: 16 (over z, y, x), tp: 2 (over core).
Axes of the slice: x: 2, y: 2, z: 4, core: 2. Of those that a mesh axis runs over, the one named last changes fastest.
Arguments:
- resid: bfloat16 [2048, 2048], P('sp'), may hold values from -6 to 6
- queries: bfloat16 [2048, 1024], P('sp', 'tp'), may hold values from -6 to 6
- keys: bfloat16 [2048, 1024], P('sp', 'tp'), may hold values from -6 to 6
- values: bfloat16 [2048, 2048], P('sp', 'tp'), may hold values from -6 to 6
- decay_pre: float32 [2048, 1024], P('sp', 'tp'), may hold values from -4 to 11.5
- out_gate: bfloat16 [2048, 2048], P('sp', 'tp'), may hold values from -6 to 6
- head_gain: float32 [256], replicated, may hold values from 0.1 to 1.9
- out_proj: bfloat16 [2048, 2048], P('tp'), may hold values from -0.25 to 0.25
- mix_gain: float32 [2048], replicated, may hold values from 0.1 to 1.9
- mix_shift: float32 [2048], replicated, may hold values from -3 to 3
- gate_in: bfloat16 [2048, 5632], P('sp', 'tp'), may hold values from -0.125 to 0.125
- up_in: bfloat16 [2048, 5632], P('sp', 'tp'), may hold values from -0.125 to 0.125
- down_out: bfloat16 [5632, 2048], P('tp', 'sp'), may hold values from -0.25 to 0.25
- out_gain: float32 [2048], replicated, may hold values from 0.1 to 1.9
- out_shift: float32 [2048], replicated, may hold values from -2 to 2
Outputs:
- result: bfloat16 [2048, 2048], P('sp')
The draws below stay inside these ranges and needn't reach their ends.
All inputs are finite; a program needn't handle non-finite values.
Results may differ from the reference program's by a relative error of at most 0.02.
Values may be sent and summed in bfloat16 or wider, within the bound.
A program may use at most 128 MiB of HBM per device.

```python
import jax
import jax.numpy as jnp
from jax import lax

D = 2048
HEADS = 8
HK = 128
HV = 256
FF = 5632
SPAN = 64
TOK_DEV = 128
TOKENS = 2048
KEYDIM = 1024
VALDIM = 2048
N_SP = 16
N_TP = 2


def draw_decay_pre(key, part):
    key_slow = jax.random.fold_in(key, 11)
    key_high = jax.random.fold_in(key, 12)
    key_low = jax.random.fold_in(key, 13)
    key_segment = jax.random.fold_in(key, 14)
    key_noise = jax.random.fold_in(key, 15)
    share = 0.5
    slow = jax.random.uniform(key_slow, (KEYDIM,), jnp.float32) < share
    keep_rate = jax.random.uniform(key_high, (KEYDIM,), jnp.float32, 0.5, 1.5)
    high = jnp.log(jnp.float32(TOKENS) / (16.0 * keep_rate))
    low = jax.random.uniform(key_low, (KEYDIM,), jnp.float32, -1.0, 1.0)
    base = jnp.where(slow, high, low)
    segment = jnp.arange(TOKENS) // TOK_DEV
    position_shifts = jax.random.uniform(key_segment, (TOKENS // TOK_DEV,), jnp.float32, -1.2, 1.2)[segment]
    noise = jnp.clip(jax.random.normal(key_noise, (TOKENS, KEYDIM), jnp.float32), -3.5, 3.5) * 0.5
    return (base[None, :] + position_shifts[:, None] + noise).astype(jnp.float32)


def shard_levels(rng, dims, shards, smallest, largest):
    loudness, own = 1.0, jax.random.fold_in(rng, 6)
    for dim, parts in shards:
        heights = jnp.exp(jax.random.uniform(jax.random.fold_in(own, dim), (parts,), jnp.float32, smallest / len(shards), largest / len(shards)))
        loudness = loudness * jnp.repeat(heights, dims[dim] // parts).reshape([-1 if axis == dim else 1 for axis in range(len(dims))])
    return loudness


def gaussian(own_key, dims, scale, most, shards=(), held_as=jnp.bfloat16):
    array = scale * jax.random.normal(own_key, dims, jnp.float32)
    if shards:
        array = array * shard_levels(own_key, dims, shards, -0.22, 0.18)
    return jnp.clip(array, -most, most).astype(held_as)


def setup_inputs(seed: int = 0) -> dict:
    arg_keys = jax.random.split(jax.random.key(seed), 16)
    resid = gaussian(arg_keys[0], (TOKENS, D), 1.0, 6.0, ((0, 16),))
    queries = gaussian(arg_keys[1], (TOKENS, KEYDIM), 1.0, 6.0, ((0, 16), (1, 2)))
    keys = gaussian(arg_keys[2], (TOKENS, KEYDIM), 1.0, 6.0, ((0, 16), (1, 2)))
    values = gaussian(arg_keys[3], (TOKENS, VALDIM), 1.0, 6.0, ((0, 16), (1, 2)))
    decay_pre = draw_decay_pre(jax.random.fold_in(arg_keys[15], 71), 0)
    out_gate = gaussian(arg_keys[5], (TOKENS, VALDIM), 1.0, 6.0, ((0, 16), (1, 2)))
    head_gain = jnp.clip(1.0 + 0.18 * jax.random.normal(arg_keys[6], (HV,), jnp.float32), 0.1, 1.9)
    out_proj = gaussian(arg_keys[7], (VALDIM, D), (VALDIM // 4) ** -0.5, 0.25, ((0, 2),))
    mix_gain = jnp.clip(1.0 + 0.18 * jax.random.normal(arg_keys[8], (D,), jnp.float32), 0.1, 1.9)
    mix_shift = gaussian(arg_keys[9], (D,), 0.5, 3.0, (), jnp.float32)
    gate_in = gaussian(arg_keys[10], (D, FF), D ** -0.5, 0.125, ((0, 16), (1, 2)))
    up_in = gaussian(arg_keys[11], (D, FF), D ** -0.5, 0.125, ((0, 16), (1, 2)))
    down_out = gaussian(arg_keys[12], (FF, D), (FF // 9) ** -0.5, 0.25, ((0, 2), (1, 16)))
    out_gain = jnp.clip(1.0 + 0.18 * jax.random.normal(arg_keys[13], (D,), jnp.float32), 0.1, 1.9)
    out_shift = gaussian(arg_keys[14], (D,), 0.3, 2.0, (), jnp.float32)
    return {"resid": resid, "queries": queries, "keys": keys, "values": values, "decay_pre": decay_pre, "out_gate": out_gate, "head_gain": head_gain, "out_proj": out_proj, "mix_gain": mix_gain, "mix_shift": mix_shift, "gate_in": gate_in, "up_in": up_in, "down_out": down_out, "out_gain": out_gain, "out_shift": out_shift}


ALPHA = 2.0 ** 0.25
LN_EPS = 1e-05
RMS_EPS = 1e-06
TAU = 16.0

def layer_norm(inputs, gain, shift):
    center = inputs - lax.optimization_barrier(jnp.mean(inputs, axis=-1, keepdims=True))
    spread = lax.optimization_barrier(jnp.mean(center * center, axis=-1, keepdims=True))
    return center * lax.rsqrt(spread + LN_EPS) * gain + shift

def group_sum(left, weight, width):
    total = jnp.zeros((left.shape[0], weight.shape[1]), jnp.float32)
    for group in range(N_TP):
        partial_sum = jnp.dot(left[:, group * width:(group + 1) * width], weight[group * width:(group + 1) * width], preferred_element_type=jnp.float32)
        rounded = lax.optimization_barrier(partial_sum.astype(jnp.bfloat16))
        total = total + rounded.astype(jnp.float32)
    return total

def reference(resid, queries, keys, values, decay_pre, out_gate, head_gain, out_proj, mix_gain, mix_shift, gate_in, up_in, down_out, out_gain, out_shift):
    blocks = TOKENS // SPAN
    logdecay = jax.nn.log_sigmoid(decay_pre) / TAU
    scaled_q = queries.astype(jnp.float32).reshape(blocks, SPAN, HEADS, HK) * HK ** (-0.5)
    key_block = keys.astype(jnp.float32).reshape(blocks, SPAN, HEADS, HK)
    value_block = values.astype(jnp.float32).reshape(blocks, SPAN, HEADS, HV)
    cumul = jnp.cumsum(logdecay.reshape(blocks, SPAN, HEADS, HK), axis=1)
    last = cumul[:, -1]
    key_decayed = key_block * jnp.exp(last[:, None] - cumul)

    def advance(running_state, inputs):
        decay_end, current_key, current_value, current_query = inputs
        state_increment = jnp.einsum('tiw,tiz->iwz', current_key, current_value, precision=lax.Precision.HIGHEST)
        running_state = jnp.exp(decay_end)[..., None] * running_state + state_increment
        return (running_state, jnp.einsum('qpy,pyr->qpr', current_query, running_state, precision=lax.Precision.HIGHEST))
    _, state_readout = lax.scan(advance, jnp.zeros((HEADS, HK, HV), jnp.float32), (last, key_decayed, value_block, scaled_q))
    state_readout = state_readout.reshape(TOKENS, HEADS, HV)
    normed = state_readout * lax.rsqrt(lax.optimization_barrier(jnp.mean(state_readout * state_readout, axis=-1, keepdims=True)) + RMS_EPS) * head_gain
    gated = (normed.reshape(TOKENS, VALDIM) * jax.nn.silu(out_gate.astype(jnp.float32))).astype(jnp.bfloat16)
    mixed = group_sum(gated, out_proj, VALDIM // N_TP)
    mid = layer_norm(ALPHA * resid.astype(jnp.float32) + mixed, mix_gain, mix_shift).astype(jnp.bfloat16)

    def channel_mix(middle_block):
        gate = jnp.dot(middle_block, gate_in, preferred_element_type=jnp.float32)
        upward = jnp.dot(middle_block, up_in, preferred_element_type=jnp.float32)
        hidden = (jax.nn.silu(gate) * upward).astype(jnp.bfloat16)
        ffn = group_sum(hidden, down_out, FF // N_TP)
        return layer_norm(ALPHA * middle_block.astype(jnp.float32) + 0.5 * ffn, out_gain, out_shift).astype(jnp.bfloat16)
    result = lax.map(channel_mix, mid.reshape(N_SP, TOK_DEV, D))
    return result.reshape(TOKENS, D)
```

```python
import functools

import jax
import jax.numpy as jnp
from jax import lax
from jax.experimental import pallas as pl
from jax.experimental.pallas import tpu as pltpu
from jax.sharding import PartitionSpec as P

HK = 128
HV = 256
SPAN = 64
LANES = 128


ALPHA = 2.0**0.25
LN_EPS = 1e-05
RMS_EPS = 1e-06
TAU = 16.0
MESH = pl.DeviceIdType.MESH


def entering(array, axis, combine, identity):
    count, place = (lax.axis_size(axis), lax.axis_index(axis))
    everything = jax.tree.map(
        lambda part, kind: lax.all_gather(part.astype(kind), axis),
        array,
        (jnp.bfloat16, jnp.bfloat16),
    )
    start = jax.tree.map(
        lambda part, zero: jnp.broadcast_to(jnp.asarray(zero, part.dtype), part.shape),
        array,
        identity,
    )

    def lap(k, before):
        reached = k < place
        new = combine(
            before, jax.tree.map(lambda part, own: part[k].astype(own.dtype), everything, array)
        )
        return jax.tree.map(lambda a, b: jnp.where(reached, a, b), new, before)

    return lax.fori_loop(0, count, lap, start)


def layer_norm(inputs, gain, shift):
    center = inputs - jnp.mean(inputs, axis=-1, keepdims=True)
    spread = jnp.mean(center * center, axis=-1, keepdims=True)
    return center * lax.rsqrt(spread + LN_EPS) * gain + shift


def combine_states(earlier, later):
    return (earlier[0] * later[0], later[0][..., None] * earlier[1] + later[1])


def greet(places):
    barrier = pltpu.get_barrier_semaphore()
    for place in places:
        pl.semaphore_signal(barrier, inc=1, device_id=place, device_id_type=MESH)
    pl.semaphore_wait(barrier, len(places))


def remote(src, dst, send, recv, place):
    return pltpu.make_async_remote_copy(
        src_ref=src, dst_ref=dst, send_sem=send, recv_sem=recv, device_id=place, device_id_type=MESH
    )


def local_tokens(queries, keys, values, decay_pre):
    tok_rows = queries.shape[0]
    local_heads = queries.shape[1] // HK
    blocks = tok_rows // SPAN
    logdecay = jax.nn.log_sigmoid(decay_pre) / TAU
    scaled_q = queries.astype(jnp.float32).reshape(blocks, SPAN, local_heads, HK) * HK ** (-0.5)
    key_block = keys.astype(jnp.float32).reshape(blocks, SPAN, local_heads, HK)
    value_block = values.astype(jnp.float32).reshape(blocks, SPAN, local_heads, HV)
    cumul = jnp.cumsum(logdecay.reshape(blocks, SPAN, local_heads, HK), axis=1)
    last = cumul[:, -1]
    key_decayed = key_block * jnp.exp(last[:, None] - cumul)
    updates = jnp.einsum(
        "nchk,nchv->nhkv", key_decayed, value_block, precision=lax.Precision.HIGHEST
    )

    def advance(running_state, inputs):
        decay_end, state_increment, current_query = inputs
        running_state = jnp.exp(decay_end)[..., None] * running_state + state_increment
        return (
            running_state,
            jnp.einsum(
                "qpy,pyr->qpr", current_query, running_state, precision=lax.Precision.HIGHEST
            ),
        )

    own_state, local_read = lax.scan(
        advance, jnp.zeros((local_heads, HK, HV), jnp.float32), (last, updates, scaled_q)
    )
    block_ends = jnp.cumsum(last, axis=0)
    own_decay = jnp.exp(block_ends[-1])
    carry_q = scaled_q * jnp.exp(block_ends)[:, None]
    return local_read, carry_q, own_decay, own_state


def mix_tokens(local_read, carry_q, own_decay, own_state, out_gate, head_gain):
    blocks, span, local_heads, _ = carry_q.shape
    tok_rows = blocks * span
    identity = (jnp.ones_like(own_decay), jnp.zeros_like(own_state))
    _, incoming = entering((own_decay, own_state), "sp", combine_states, identity)
    carried = jnp.einsum(
        "xepj,pjw->xepw", carry_q, incoming, precision=lax.Precision.HIGHEST
    )
    state_readout = (local_read + carried).reshape(tok_rows, local_heads, HV)
    normed = (
        state_readout
        * lax.rsqrt(jnp.mean(state_readout * state_readout, axis=-1, keepdims=True) + RMS_EPS)
        * head_gain
    )
    return (
        normed.reshape(tok_rows, local_heads * HV) * jax.nn.silu(out_gate.astype(jnp.float32))
    ).astype(jnp.bfloat16)


def hidden_by_rows(whole_rows, gate_in, up_in):
    gate = jnp.dot(
        whole_rows,
        lax.all_gather(gate_in, "sp", axis=0, tiled=True),
        preferred_element_type=jnp.float32,
    )
    upward = jnp.dot(
        whole_rows,
        lax.all_gather(up_in, "sp", axis=0, tiled=True),
        preferred_element_type=jnp.float32,
    )
    return (jax.nn.silu(gate) * upward).astype(jnp.bfloat16)


def down_by_columns(hidden, down_out):
    return jnp.dot(
        hidden,
        lax.all_gather(down_out, "sp", axis=1, tiled=True),
        preferred_element_type=jnp.float32,
    )


def layer_kernel(
    deep,
    wide,
    queries,
    keys,
    values,
    decay_pre,
    out_gate,
    head_gain,
    out_proj,
    resid,
    mix_gain,
    mix_shift,
    gate_in,
    up_in,
    down_out,
    gain,
    shift,
    out,
    w1,
    w2,
    proj,
    updates,
    ends,
    s_out,
    d_out,
    s_in,
    d_in,
    before,
    total,
    t_out,
    t_in,
    dt_out,
    dt_in,
    s_start,
    start,
    gated,
    mixed,
    mixed_in,
    rows,
    hidden,
    part,
    y_in,
    u_in,
    v_in,
    z_out,
    acc,
    own_sem,
    b_send,
    b_recv,
    f_send,
    f_recv,
    t_send,
    t_recv,
    p1_send,
    p1_recv,
    p2_send,
    p2_recv,
    p3_send,
    p3_recv,
    m_sem,
    au_send,
    av_send,
    ay_send,
    az_recv,
    ay_recv,
    ry_send,
    ry_recv,
    rz_send,
    ru_recv,
    rv_recv,
    f_sem,
):
    me, core = lax.axis_index("sp"), lax.axis_index("tp")
    x, y, z = me % 2, (me // 2) % 2, me // 4
    group = me // 2
    groups = 2 * deep
    plane = 4
    place = me % plane
    own, inner = rows.shape[2], rows.shape[3]
    depth = gate_in.shape[0]
    lanes = down_out.shape[1]
    span = wide * LANES
    half = lambda c: pl.ds(pl.multiple_of(c * span, span), span)
    twin = (me, 1 - core)
    x_place = (me + 1 - 2 * x, core)
    y_place = (me + 2 - 4 * y, core)
    above, below = (me + plane, core), (me - plane, core)
    sides = [(dy, dz) for dz in range(deep) for dy in range(2)]

    def at(xx, yy, zz):
        return (plane * zz + 2 * yy + xx, core)

    def target(r):
        dy, dz = sides[r]
        return (y + dy) % 2, (z + dz) % deep

    def origin(r):
        dy, dz = sides[r]
        return (y + dy) % 2, (z + deep - dz) % deep

    def fellow(dp):
        return (x + dp % 2) % 2, (y + dp // 2) % 2

    def short(c, g):
        return jnp.logical_or(g == c, g == groups - 2 + c)

    def first_block(c, g):
        return wide * g - (g > c).astype(jnp.int32) - (g > groups - 2 + c).astype(jnp.int32)

    def sized(flag, run):
        @pl.when(flag)
        def _():
            run(wide - 1)

        @pl.when(jnp.logical_not(flag))
        def _():
            run(wide)

    def taken(mat, g, blocks):
        begin = pl.ds(pl.multiple_of(first_block(core, g) * LANES, LANES), blocks * LANES)
        return (gate_in.at[:, begin], up_in.at[:, begin], down_out.at[begin])[mat]

    def landing(mat, c, s, blocks):
        if mat < 2:
            rows_of = pl.ds(pl.multiple_of(s * depth, depth), depth)
            return w1.at[c, rows_of, pl.ds(mat * span, blocks * LANES)]
        columns = pl.ds(pl.multiple_of(s * lanes, lanes), lanes)
        return w2.at[pl.ds(pl.multiple_of(c * span, span), blocks * LANES), columns]

    def slab(j, c, s):
        if j == 0:
            return w1.at[c, pl.ds(pl.multiple_of(s * depth, depth), depth)]
        return landing(2, c, s, wide)

    def bring(mat, r, run):
        yy, zz = target(r)
        goal = at(x, yy, zz) if r else x_place
        g = 2 * zz + yy

        def copy(blocks):
            run(
                remote(
                    taken(mat, g, blocks),
                    landing(mat, core, me, blocks),
                    b_send.at[mat, r],
                    b_recv.at[mat, r],
                    goal,
                )
            )

        sized(short(core, g), copy)

    def send(mat, *which):
        for r in which:
            bring(mat, r, lambda copy: copy.start())

    def relay(mat, r):
        yy, zz = origin(r)
        s = plane * zz + 2 * yy + x
        block = landing(mat, core, s, wide)
        return remote(block, block, f_send.at[mat, r], f_recv.at[mat, r], x_place)

    def share(j, k, r):
        yy, zz = origin(r)
        s = plane * zz + 2 * yy + (x + k) % 2
        block = slab(j, core, s)
        return remote(block, block, t_send.at[j, k, r], t_recv.at[j, k, r], twin)

    def came(ref, sem):
        remote(ref, ref, f_sem.at[0], sem, twin).wait_recv()

    def shared(mat, k, r):
        if mat:
            share(mat - 1, k, r).start()

    def pass_on(mat, *which):
        for r in which:
            yy, zz = origin(r)
            s = plane * zz + 2 * yy + x if r else x_place[0]
            sized(
                short(core, group),
                lambda blocks, s=s, r=r: came(landing(mat, core, s, blocks), b_recv.at[mat, r]),
            )
            if r:
                relay(mat, r).start()
            shared(mat, 0 if r else 1, r)

    def passed(mat, *which):
        for r in which:
            yy, zz = origin(r)
            came(landing(mat, core, plane * zz + 2 * yy + (1 - x), wide), f_recv.at[mat, r])
            shared(mat, 1, r)

    def local(mat, run):
        def copy(blocks):
            run(
                pltpu.make_async_copy(
                    taken(mat, group, blocks), landing(mat, core, me, blocks), own_sem.at[mat]
                )
            )

        sized(short(core, group), copy)

    pure_z = [r for r, (dy, dz) in enumerate(sides) if not dy and dz]
    cross = [r for r, (dy, dz) in enumerate(sides) if dy and dz]
    near = [0, 1]
    keep_proj = pltpu.make_async_copy(out_proj, proj, own_sem.at[3])

    last_block = (wide - 1) * LANES
    w1[core, :, last_block:span] = jnp.zeros((w1.shape[1], LANES), jnp.bfloat16)
    w1[core, :, span + last_block :] = jnp.zeros((w1.shape[1], LANES), jnp.bfloat16)
    tail = pl.ds(pl.multiple_of(core * span + last_block, LANES), LANES)
    w2[tail] = jnp.zeros((LANES, inner), jnp.bfloat16)

    with jax.named_scope("greet"):
        partners = [at(x, *target(r)) for r in range(1, 2 * deep)]
        partners += [x_place, at(*fellow(3), z), twin]
        greet(partners)
    send(0, *pure_z)
    for mat in range(3):
        local(mat, lambda copy: copy.start())
    keep_proj.start()

    with jax.named_scope("local"):
        tokens = queries.shape[0]
        heads = queries.shape[1] // HK
        blocks = tokens // SPAN
        raw = decay_pre[...]
        logdecay = (jnp.minimum(raw, 0.0) - jnp.log1p(jnp.exp(-jnp.abs(raw)))) / TAU
        row = lax.broadcasted_iota(jnp.int32, (tokens, tokens), 0)
        col = lax.broadcasted_iota(jnp.int32, (tokens, tokens), 1)
        tri = jnp.logical_and(row // SPAN == col // SPAN, col <= row).astype(jnp.float32)
        cumul = jnp.dot(
            tri, logdecay, precision=lax.Precision.HIGHEST, preferred_element_type=jnp.float32
        )
        lasts = [cumul[(n + 1) * SPAN - 1 : (n + 1) * SPAN] for n in range(blocks)]
        across = (((0,), (0,)), ((), ()))

        def column(line):
            return jnp.broadcast_to(line, (HK, HK)).T

        def spread(square):
            return jnp.concatenate([square] * (HV // HK), axis=1)

        for n in range(blocks):
            steps = slice(n * SPAN, (n + 1) * SPAN)
            faded = keys[steps].astype(jnp.float32) * jnp.exp(lasts[n] - cumul[steps])
            high = faded.astype(jnp.bfloat16)
            low = (faded - high.astype(jnp.float32)).astype(jnp.bfloat16)
            for h in range(heads):
                key = slice(h * HK, (h + 1) * HK)
                value = values[steps, h * HV : (h + 1) * HV]
                updates[n, h] = lax.dot_general(
                    high[:, key], value, across, preferred_element_type=jnp.float32
                ) + lax.dot_general(
                    low[:, key], value, across, preferred_element_type=jnp.float32
                )
                ends[n, h] = column(jnp.exp(lasts[n][:, key]))
        whole = jnp.exp(sum(lasts))
        for h in range(heads):
            state = updates[0, h]
            for n in range(1, blocks):
                state = spread(ends[n, h]) * state + updates[n, h]
            s_out[h] = state.astype(jnp.bfloat16)
            d_out[h] = jnp.broadcast_to(whole[:, h * HK : (h + 1) * HK], d_out.shape[1:])

    def to_plane(dp):
        xx, yy = fellow(dp)
        goal, slot = at(xx, yy, z), 2 * yy + xx
        return (
            remote(s_out.at[slot], s_in.at[place], p1_send.at[dp, 0], p1_recv.at[dp, 0], goal),
            remote(d_out.at[slot], d_in.at[place], p1_send.at[dp, 1], p1_recv.at[dp, 1], goal),
        )

    for dp in range(1, plane):
        for copy in to_plane(dp):
            copy.start()
    s_in[place] = s_out[place]
    d_in[place] = d_out[place]
    send(0, *near)

    with jax.named_scope("p1"):
        for dp in range(1, plane):
            for copy in to_plane(dp):
                copy.wait_recv()
    running = jnp.zeros((HK, HV), jnp.float32)
    line = jnp.ones((1, HK), jnp.float32)
    reach = []
    for i in range(plane):
        before[i] = running
        reach.append(line)
        own_decay = d_in[i][:1]
        running = spread(column(own_decay)) * running + s_in[i].astype(jnp.float32)
        line = line * own_decay
    t_out[...] = running.astype(jnp.bfloat16)
    dt_out[...] = jnp.broadcast_to(line, dt_out.shape)

    def to_later(zz):
        goal = at(x, y, zz)
        return (
            remote(t_out, t_in.at[z], p2_send.at[zz, 0], p2_recv.at[z, 0], goal),
            remote(dt_out, dt_in.at[z], p2_send.at[zz, 1], p2_recv.at[z, 1], goal),
        )

    for zz in range(1, deep):

        @pl.when(zz > z)
        def _():
            for copy in to_later(zz):
                copy.start()

    send(0, *cross)
    send(1, *pure_z)
    with jax.named_scope("gates1"):
        pass_on(0, *pure_z)
    total[...] = jnp.zeros(total.shape, jnp.float32)
    with jax.named_scope("p2"):
        for zz in range(deep - 1):

            @pl.when(zz < z)
            def _():
                came(t_in.at[zz], p2_recv.at[zz, 0])
                came(dt_in.at[zz], p2_recv.at[zz, 1])
                fade = spread(column(dt_in[zz][:1]))
                total[...] = fade * total[...] + t_in[zz].astype(jnp.float32)

    for i in range(plane):
        s_start[i] = (before[i] + spread(column(reach[i])) * total[...]).astype(jnp.bfloat16)

    def to_fellow(dp):
        xx, yy = fellow(dp)
        slot = 2 * yy + xx
        return remote(
            s_start.at[slot], start.at[place], p3_send.at[dp], p3_recv.at[dp], at(xx, yy, z)
        )

    for dp in range(1, plane):
        to_fellow(dp).start()
    start[place] = s_start[place]
    send(1, *near)
    with jax.named_scope("gates2"):
        pass_on(0, *near)
    with jax.named_scope("p3"):
        for dp in range(1, plane):
            to_fellow(dp).wait_recv()

    with jax.named_scope("mix"):
        for h in range(heads):
            thick = slice(h * HV, (h + 1) * HV)
            state = start[h].astype(jnp.float32)
            reads = []
            for n in range(blocks):
                state = spread(ends[n, h]) * state + updates[n, h]
                high = state.astype(jnp.bfloat16)
                low = (state - high.astype(jnp.float32)).astype(jnp.bfloat16)
                query = queries[n * SPAN : (n + 1) * SPAN, h * HK : (h + 1) * HK]
                reads.append(
                    jnp.dot(query, high, preferred_element_type=jnp.float32)
                    + jnp.dot(query, low, preferred_element_type=jnp.float32)
                )
            read = jnp.concatenate(reads, axis=0) * HK ** (-0.5)
            size = jnp.mean(read * read, axis=-1, keepdims=True)
            pre = out_gate[:, thick].astype(jnp.float32)
            normed = read * lax.rsqrt(size + RMS_EPS) * head_gain[...]
            gated[:, thick] = (normed * (pre * jax.nn.sigmoid(pre))).astype(jnp.bfloat16)
    keep_proj.wait()
    with jax.named_scope("proj"):
        summed_heads = jnp.dot(gated[...], proj[...], preferred_element_type=jnp.float32)
        mixed[...] = summed_heads.astype(jnp.bfloat16).reshape(2, own, inner)
    swap = remote(mixed.at[1 - core], mixed_in, m_sem.at[0], m_sem.at[1], twin)
    swap.start()
    with jax.named_scope("swap"):
        swap.wait()
    with jax.named_scope("ln"):
        added = mixed[core].astype(jnp.float32) + mixed_in[...].astype(jnp.float32)
        middle = ALPHA * resid[core].astype(jnp.float32) + added
        rows[y, z] = layer_norm(middle, mix_gain[...], mix_shift[...]).astype(jnp.bfloat16)

    def climb(zz):
        block = rows.at[y, zz]
        return remote(block, block, au_send.at[zz], az_recv.at[zz], above)

    def sink(zz):
        block = rows.at[y, zz]
        return remote(block, block, av_send.at[zz], az_recv.at[zz], below)

    def cross_y(zz):
        block = rows.at[y, zz]
        return remote(block, block, ay_send.at[zz], ay_recv.at[zz], y_place)

    @pl.when(z < deep - 1)
    def _():
        climb(z).start()

    @pl.when(z > 0)
    def _():
        sink(z).start()

    cross_y(z).start()
    send(1, *cross)
    send(2, *pure_z)

    def landed(far):
        @pl.when(z >= far)
        def _():
            came(rows.at[y, z - far], az_recv.at[z - far])

            @pl.when(z < deep - 1)
            def _():
                climb(z - far).start()

            cross_y(z - far).start()

        @pl.when(z < deep - far)
        def _():
            came(rows.at[y, z + far], az_recv.at[z + far])

            @pl.when(z > 0)
            def _():
                sink(z + far).start()

            cross_y(z + far).start()

    with jax.named_scope("wa"):
        for mat in range(3):
            local(mat, lambda copy: copy.wait())
        share(0, 0, 0).start()
        share(1, 0, 0).start()
        pass_on(0, *cross)
        pass_on(1, *near)
        pass_on(1, *pure_z)
    with jax.named_scope("ag1"):
        landed(1)
    send(2, *near)
    send(2, *cross)
    with jax.named_scope("wb"):
        passed(0, *range(1, 2 * deep))
    with jax.named_scope("ag2"):
        landed(2)
    with jax.named_scope("wc"):
        pass_on(1, *cross)
    with jax.named_scope("ag3"):
        for far in range(3, deep):
            landed(far)
    with jax.named_scope("wd"):
        pass_on(2, *near)
        pass_on(2, *pure_z)
        passed(1, *range(1, 2 * deep))
    with jax.named_scope("agy"):
        for zz in range(deep):
            came(rows.at[1 - y, zz], ay_recv.at[zz])
    with jax.named_scope("we"):
        for k in range(2):
            for r in range(2 * deep):
                yy, zz = origin(r)
                s = plane * zz + 2 * yy + (x + k) % 2
                came(slab(0, 1 - core, s), t_recv.at[0, k, r])

    def hide(side, slot):
        left = rows[side].reshape(deep * own, inner)
        for c in range(2):
            both = jnp.dot(left, w1[c], preferred_element_type=jnp.float32)
            gate, up = both[:, :span], both[:, span:]
            hidden[slot, :, c * span : (c + 1) * span] = (
                gate * jax.nn.sigmoid(gate) * up
            ).astype(jnp.bfloat16)

    def lower(side, slot):
        down = jnp.dot(hidden[slot], w2[...], preferred_element_type=jnp.float32)
        part[side] = down.astype(jnp.bfloat16).reshape(deep, own, inner)

    with jax.named_scope("hide0"):
        hide(1 - y, 0)
    with jax.named_scope("wf"):
        pass_on(2, *cross)
    with jax.named_scope("hide1"):
        hide(y, 1)
    with jax.named_scope("wg"):
        passed(2, *range(1, 2 * deep))
        for k in range(2):
            for r in range(2 * deep):
                yy, zz = origin(r)
                s = plane * zz + 2 * yy + (x + k) % 2
                came(slab(1, 1 - core, s), t_recv.at[1, k, r])

    low_side = z < deep // 2
    order = [
        jnp.where(low_side, deep - 1, 0),
        jnp.where(low_side, deep - 2, 1),
        jnp.where(low_side, 1 - z, 2 * deep - 3 - z),
        z,
    ]

    def across_y(d):
        return remote(part.at[1 - y, d], y_in.at[d], ry_send.at[d], ry_recv.at[d], y_place)

    def hop(i, up):
        d = order[i]
        into, sem = (u_in, ru_recv) if up else (v_in, rv_recv)
        return remote(z_out.at[i], into.at[d], rz_send.at[i], sem.at[d], above if up else below)

    with jax.named_scope("down0"):
        lower(1 - y, 0)
    for d in order:
        across_y(d).start()
    with jax.named_scope("down1"):
        lower(y, 1)

    def gather_in(d, from_below, from_above):
        came(y_in.at[d], ry_recv.at[d])
        acc[...] = part[y, d].astype(jnp.float32) + y_in[d].astype(jnp.float32)

        @pl.when(from_below)
        def _():
            came(u_in.at[d], ru_recv.at[d])
            acc[...] += u_in[d].astype(jnp.float32)

        @pl.when(from_above)
        def _():
            came(v_in.at[d], rv_recv.at[d])
            acc[...] += v_in[d].astype(jnp.float32)

    for i in range(deep - 1):
        with jax.named_scope(f"rs{i}"):
            d = order[i]
            up = d > z
            gather_in(
                d,
                jnp.logical_and(up, z > 0),
                jnp.logical_and(jnp.logical_not(up), z < deep - 1),
            )
            z_out[i] = acc[...].astype(jnp.bfloat16)

            @pl.when(up)
            def _():
                hop(i, True).start()

            @pl.when(jnp.logical_not(up))
            def _():
                hop(i, False).start()

    with jax.named_scope("rsend"):
        gather_in(z, z > 0, z < deep - 1)
    with jax.named_scope("fin"):
        finished = layer_norm(
            ALPHA * rows[y, z].astype(jnp.float32) + 0.5 * acc[...], gain[...], shift[...]
        )
        out[core] = finished.astype(jnp.bfloat16)
    last = remote(out.at[core], out.at[core], f_sem.at[0], f_sem.at[1], twin)
    last.start()

    with jax.named_scope("drain"):
        for mat in range(3):
            for r in range(2 * deep):
                bring(mat, r, lambda copy: copy.wait_send())
                if r:
                    relay(mat, r).wait_send()
        for j in range(2):
            for k in range(2):
                for r in range(2 * deep):
                    share(j, k, r).wait_send()
        for dp in range(1, plane):
            for copy in (*to_plane(dp), to_fellow(dp)):
                copy.wait_send()
        for zz in range(deep):

            @pl.when(zz > z)
            def _():
                for copy in to_later(zz):
                    copy.wait_send()

            @pl.when(jnp.logical_and(zz <= z, z < deep - 1))
            def _():
                climb(zz).wait_send()

            @pl.when(jnp.logical_and(zz >= z, z > 0))
            def _():
                sink(zz).wait_send()

            cross_y(zz).wait_send()
            across_y(zz).wait_send()
        for i in range(deep - 1):
            hop(i, True).wait_send()
        last.wait()


def layer(
    resid,
    queries,
    keys,
    values,
    decay_pre,
    out_gate,
    head_gain,
    out_proj,
    mix_gain,
    mix_shift,
    gate_in,
    up_in,
    down_out,
    gain,
    shift,
):
    count = lax.axis_size("sp")
    tok_rows, inner = resid.shape
    own = tok_rows // 2
    deep = count // 4
    groups = count // 2
    wide = -(-(gate_in.shape[1] // LANES) // groups)
    span = wide * LANES
    heads = queries.shape[1] // HK
    steps = tok_rows // SPAN
    dma = pltpu.SemaphoreType.DMA
    half, full = jnp.bfloat16, jnp.float32
    block = lambda *lead: pltpu.VMEM((*lead, own, inner), half)
    near, far = pl.BlockSpec(memory_space=pltpu.VMEM), pl.BlockSpec(memory_space=pl.ANY)
    out = pl.pallas_call(
        functools.partial(layer_kernel, deep, wide),
        out_shape=jax.ShapeDtypeStruct((2, own, inner), half),
        in_specs=[near] * 6 + [far] + [near] * 3 + [far] * 3 + [near] * 2,
        out_specs=near,
        scratch_shapes=[
            pltpu.VMEM((2, inner, 2 * span), half),
            pltpu.VMEM((2 * span, inner), half),
            pltpu.VMEM(out_proj.shape, half),
            pltpu.VMEM((steps, heads, HK, HV), full),
            pltpu.VMEM((steps, heads, HK, HK), full),
            pltpu.VMEM((heads, HK, HV), half),
            pltpu.VMEM((heads, 8, HK), full),
            pltpu.VMEM((4, HK, HV), half),
            pltpu.VMEM((4, 8, HK), full),
            pltpu.VMEM((4, HK, HV), full),
            pltpu.VMEM((HK, HV), full),
            pltpu.VMEM((HK, HV), half),
            pltpu.VMEM((deep, HK, HV), half),
            pltpu.VMEM((8, HK), full),
            pltpu.VMEM((deep, 8, HK), full),
            pltpu.VMEM((4, HK, HV), half),
            pltpu.VMEM((4, HK, HV), half),
            pltpu.VMEM((tok_rows, out_proj.shape[0]), half),
            block(2),
            block(),
            block(2, deep),
            pltpu.VMEM((2, deep * own, 2 * span), half),
            block(2, deep),
            block(deep),
            block(deep),
            block(deep),
            block(deep - 1),
            pltpu.VMEM((own, inner), full),
            dma((4,)),
            dma((3, groups)),
            dma((3, groups)),
            dma((3, groups)),
            dma((3, groups)),
            dma((2, 2, groups)),
            dma((2, 2, groups)),
            dma((4, 2)),
            dma((4, 2)),
            dma((deep, 2)),
            dma((deep, 2)),
            dma((4,)),
            dma((4,)),
            dma((2,)),
            dma((deep,)),
            dma((deep,)),
            dma((deep,)),
            dma((deep,)),
            dma((deep,)),
            dma((deep,)),
            dma((deep,)),
            dma((deep,)),
            dma((deep,)),
            dma((deep,)),
            dma((2,)),
        ],
        compiler_params=pltpu.CompilerParams(
            collective_id=2, has_side_effects=True, vmem_limit_bytes=60 * 1024 * 1024
        ),
    )(
        queries,
        keys,
        values,
        decay_pre,
        out_gate,
        head_gain[None],
        out_proj,
        resid.reshape(2, own, inner),
        mix_gain[None],
        mix_shift[None],
        gate_in,
        up_in,
        down_out,
        gain[None],
        shift[None],
    )
    return out.reshape(tok_rows, inner)


def body(
    resid,
    queries,
    keys,
    values,
    decay_pre,
    out_gate,
    head_gain,
    out_proj,
    mix_gain,
    mix_shift,
    gate_in,
    up_in,
    down_out,
    out_gain,
    out_shift,
):
    tp_count = lax.axis_size("tp")
    tok_rows = queries.shape[0]
    own_count = tok_rows // tp_count
    sp_count = lax.axis_size("sp")
    units = gate_in.shape[1]
    heads = queries.shape[1] // HK
    groups = sp_count // 2
    unit_blocks = units // LANES
    by_units = (
        tp_count == 2
        and sp_count == 16
        and heads == 4
        and units % LANES == 0
        and unit_blocks % groups == groups - 2
        and gate_in.shape[0] % LANES == 0
        and down_out.shape[1] % LANES == 0
        and gate_in.shape[0] * sp_count == resid.shape[1]
        and own_count % 16 == 0
        and tok_rows % SPAN == 0
    )
    if by_units:
        return layer(
            resid,
            queries,
            keys,
            values,
            decay_pre,
            out_gate,
            head_gain,
            out_proj,
            mix_gain,
            mix_shift,
            gate_in,
            up_in,
            down_out,
            out_gain,
            out_shift,
        )
    local = local_tokens(queries, keys, values, decay_pre)
    gated = mix_tokens(*local, out_gate, head_gain)
    mixed = lax.psum_scatter(
        jnp.dot(gated, out_proj, preferred_element_type=jnp.float32).astype(jnp.bfloat16),
        "tp",
        scatter_dimension=0,
        tiled=True,
    ).astype(jnp.float32)
    own_resid = lax.dynamic_slice_in_dim(resid, lax.axis_index("tp") * own_count, own_count, 0)
    mid = layer_norm(ALPHA * own_resid.astype(jnp.float32) + mixed, mix_gain, mix_shift).astype(
        jnp.bfloat16
    )
    whole_rows = lax.all_gather(mid, "tp", axis=0, tiled=True)
    hidden = hidden_by_rows(whole_rows, gate_in, up_in)
    ffn = lax.psum_scatter(
        down_by_columns(hidden, down_out).astype(jnp.bfloat16),
        "tp",
        scatter_dimension=0,
        tiled=True,
    ).astype(jnp.float32)
    finished = layer_norm(ALPHA * mid.astype(jnp.float32) + 0.5 * ffn, out_gain, out_shift).astype(
        jnp.bfloat16
    )
    return lax.all_gather(finished, "tp", axis=0, tiled=True)


def solution(mesh):
    return jax.shard_map(
        body,
        mesh=mesh,
        in_specs=(
            P("sp", None),
            P("sp", "tp"),
            P("sp", "tp"),
            P("sp", "tp"),
            P("sp", "tp"),
            P("sp", "tp"),
            P(),
            P("tp", None),
            P(),
            P(),
            P("sp", "tp"),
            P("sp", "tp"),
            P("tp", "sp"),
            P(),
            P(),
        ),
        out_specs=P("sp", None),
        check_vma=False,
    )
```

```python
import functools

import jax
import jax.numpy as jnp
from jax import lax
from jax.experimental import pallas as pl
from jax.experimental.pallas import tpu as pltpu
from jax.sharding import PartitionSpec as P

HK = 128
HV = 256
SPAN = 64
LANES = 128


ALPHA = 2.0**0.25
LN_EPS = 1e-05
RMS_EPS = 1e-06
TAU = 16.0
MESH = pl.DeviceIdType.MESH


def entering(array, axis, combine, identity):
    count, place = (lax.axis_size(axis), lax.axis_index(axis))
    everything = jax.tree.map(
        lambda part, kind: lax.all_gather(part.astype(kind), axis),
        array,
        (jnp.bfloat16, jnp.bfloat16),
    )
    start = jax.tree.map(
        lambda part, zero: jnp.broadcast_to(jnp.asarray(zero, part.dtype), part.shape),
        array,
        identity,
    )

    def lap(k, before):
        reached = k < place
        new = combine(
            before, jax.tree.map(lambda part, own: part[k].astype(own.dtype), everything, array)
        )
        return jax.tree.map(lambda a, b: jnp.where(reached, a, b), new, before)

    return lax.fori_loop(0, count, lap, start)


def layer_norm(inputs, gain, shift):
    center = inputs - jnp.mean(inputs, axis=-1, keepdims=True)
    spread = jnp.mean(center * center, axis=-1, keepdims=True)
    return center * lax.rsqrt(spread + LN_EPS) * gain + shift


def combine_states(earlier, later):
    return (earlier[0] * later[0], later[0][..., None] * earlier[1] + later[1])


def greet(places):
    barrier = pltpu.get_barrier_semaphore()
    for place in places:
        pl.semaphore_signal(barrier, inc=1, device_id=place, device_id_type=MESH)
    pl.semaphore_wait(barrier, len(places))


def remote(src, dst, send, recv, place):
    return pltpu.make_async_remote_copy(
        src_ref=src, dst_ref=dst, send_sem=send, recv_sem=recv, device_id=place, device_id_type=MESH
    )


def local_tokens(queries, keys, values, decay_pre):
    tok_rows = queries.shape[0]
    local_heads = queries.shape[1] // HK
    blocks = tok_rows // SPAN
    logdecay = jax.nn.log_sigmoid(decay_pre) / TAU
    scaled_q = queries.astype(jnp.float32).reshape(blocks, SPAN, local_heads, HK) * HK ** (-0.5)
    key_block = keys.astype(jnp.float32).reshape(blocks, SPAN, local_heads, HK)
    value_block = values.astype(jnp.float32).reshape(blocks, SPAN, local_heads, HV)
    cumul = jnp.cumsum(logdecay.reshape(blocks, SPAN, local_heads, HK), axis=1)
    last = cumul[:, -1]
    key_decayed = key_block * jnp.exp(last[:, None] - cumul)
    updates = jnp.einsum(
        "nchk,nchv->nhkv", key_decayed, value_block, precision=lax.Precision.HIGHEST
    )

    def advance(running_state, inputs):
        decay_end, state_increment, current_query = inputs
        running_state = jnp.exp(decay_end)[..., None] * running_state + state_increment
        return (
            running_state,
            jnp.einsum(
                "qpy,pyr->qpr", current_query, running_state, precision=lax.Precision.HIGHEST
            ),
        )

    own_state, local_read = lax.scan(
        advance, jnp.zeros((local_heads, HK, HV), jnp.float32), (last, updates, scaled_q)
    )
    block_ends = jnp.cumsum(last, axis=0)
    own_decay = jnp.exp(block_ends[-1])
    carry_q = scaled_q * jnp.exp(block_ends)[:, None]
    return local_read, carry_q, own_decay, own_state


def mix_tokens(local_read, carry_q, own_decay, own_state, out_gate, head_gain):
    blocks, span, local_heads, _ = carry_q.shape
    tok_rows = blocks * span
    identity = (jnp.ones_like(own_decay), jnp.zeros_like(own_state))
    _, incoming = entering((own_decay, own_state), "sp", combine_states, identity)
    carried = jnp.einsum(
        "xepj,pjw->xepw", carry_q, incoming, precision=lax.Precision.HIGHEST
    )
    state_readout = (local_read + carried).reshape(tok_rows, local_heads, HV)
    normed = (
        state_readout
        * lax.rsqrt(jnp.mean(state_readout * state_readout, axis=-1, keepdims=True) + RMS_EPS)
        * head_gain
    )
    return (
        normed.reshape(tok_rows, local_heads * HV) * jax.nn.silu(out_gate.astype(jnp.float32))
    ).astype(jnp.bfloat16)


def hidden_by_rows(whole_rows, gate_in, up_in):
    gate = jnp.dot(
        whole_rows,
        lax.all_gather(gate_in, "sp", axis=0, tiled=True),
        preferred_element_type=jnp.float32,
    )
    upward = jnp.dot(
        whole_rows,
        lax.all_gather(up_in, "sp", axis=0, tiled=True),
        preferred_element_type=jnp.float32,
    )
    return (jax.nn.silu(gate) * upward).astype(jnp.bfloat16)


def down_by_columns(hidden, down_out):
    return jnp.dot(
        hidden,
        lax.all_gather(down_out, "sp", axis=1, tiled=True),
        preferred_element_type=jnp.float32,
    )


def layer_kernel(
    deep,
    wide,
    queries,
    keys,
    values,
    decay_pre,
    out_gate,
    head_gain,
    out_proj,
    resid,
    mix_gain,
    mix_shift,
    gate_in,
    up_in,
    down_out,
    gain,
    shift,
    out,
    w1,
    w2,
    proj,
    updates,
    ends,
    s_out,
    d_out,
    s_in,
    d_in,
    before,
    total,
    t_out,
    t_in,
    s_start,
    start,
    gated,
    mixed,
    mixed_in,
    rows,
    hidden,
    part,
    y_in,
    u_in,
    v_in,
    z_out,
    acc,
    own_sem,
    b_send,
    b_recv,
    f_send,
    f_recv,
    t_send,
    t_recv,
    p1_send,
    p1_recv,
    p2_sem,
    p3_send,
    p3_recv,
    m_sem,
    au_send,
    av_send,
    ay_send,
    az_recv,
    ay_recv,
    ry_send,
    ry_recv,
    rz_send,
    ru_recv,
    rv_recv,
    f_sem,
    go_sem,
):
    me, core = lax.axis_index("sp"), lax.axis_index("tp")
    x, y, z = me % 2, (me // 2) % 2, me // 4
    group = me // 2
    groups = 2 * deep
    plane = 4
    place = me % plane
    own, inner = rows.shape[2], rows.shape[3]
    depth = gate_in.shape[0]
    lanes = down_out.shape[1]
    span = wide * LANES
    half = lambda c: pl.ds(pl.multiple_of(c * span, span), span)
    twin = (me, 1 - core)
    x_place = (me + 1 - 2 * x, core)
    y_place = (me + 2 - 4 * y, core)
    above, below = (me + plane, core), (me - plane, core)
    sides = [(dy, dz) for dz in range(deep) for dy in range(2)]
    bottom = z < deep // 2
    edge = jnp.logical_or(z == 0, z == deep - 1)
    pair = z + 1 - 2 * (z % 2)
    inner_z = jnp.where(bottom, deep // 2, deep // 2 - 1)
    edge_z = jnp.where(bottom, deep - 1, 0)

    def at(xx, yy, zz):
        return (plane * zz + 2 * yy + xx, core)

    def target(dy, dz):
        return (y + dy) % 2, (z + dz) % deep

    def origin(dy, dz):
        return (y + dy) % 2, (z + deep - dz) % deep

    def fellow(dp):
        return (x + dp % 2) % 2, (y + dp // 2) % 2

    def short(c, g):
        return jnp.logical_or(g == c, g == groups - 2 + c)

    def first_block(c, g):
        return wide * g - (g > c).astype(jnp.int32) - (g > groups - 2 + c).astype(jnp.int32)

    def sized(flag, run):
        @pl.when(flag)
        def _():
            run(wide - 1)

        @pl.when(jnp.logical_not(flag))
        def _():
            run(wide)

    def taken(mat, g, blocks):
        begin = pl.ds(pl.multiple_of(first_block(core, g) * LANES, LANES), blocks * LANES)
        return (gate_in.at[:, begin], up_in.at[:, begin], down_out.at[begin])[mat]

    def landing(mat, c, s, blocks):
        if mat < 2:
            rows_of = pl.ds(pl.multiple_of(s * depth, depth), depth)
            return w1.at[c, rows_of, pl.ds(mat * span, blocks * LANES)]
        columns = pl.ds(pl.multiple_of(s * lanes, lanes), lanes)
        return w2.at[pl.ds(pl.multiple_of(c * span, span), blocks * LANES), columns]

    def slab(j, c, s):
        if j == 0:
            return w1.at[c, pl.ds(pl.multiple_of(s * depth, depth), depth)]
        return landing(2, c, s, wide)

    def home(dy, dz):
        return isinstance(dz, int) and dy == 0 and dz == 0

    def bring(mat, dy, dz, run):
        yy, zz = target(dy, dz)
        goal = x_place if home(dy, dz) else at(x, yy, zz)
        g = 2 * zz + yy
        r = 2 * dz + dy

        def copy(blocks):
            run(
                remote(
                    taken(mat, g, blocks),
                    landing(mat, core, me, blocks),
                    b_send.at[mat, r],
                    b_recv.at[mat, r],
                    goal,
                )
            )

        sized(short(core, g), copy)

    def send(mat, dy, dz):
        bring(mat, dy, dz, lambda copy: copy.start())

    def send_near(mat):
        send(mat, 0, 0)
        send(mat, 1, 0)

    def send_to(mat, dy, zz):
        send(mat, dy, (zz + deep - z) % deep)

    def source(dy, dz, k):
        yy, zz = origin(dy, dz)
        return plane * zz + 2 * yy + (x + k) % 2

    def relay(mat, dy, dz, run):
        r = 2 * dz + dy

        def copy(blocks):
            block = landing(mat, core, source(dy, dz, 0), blocks)
            run(remote(block, block, f_send.at[mat, r], f_recv.at[mat, r], x_place))

        sized(short(core, group), copy)

    def share(j, k, dy, dz):
        block = slab(j, core, source(dy, dz, k))
        r = 2 * dz + dy
        return remote(block, block, t_send.at[j, k, r], t_recv.at[j, k, r], twin)

    def came(ref, sem):
        remote(ref, ref, f_sem.at[0, 0], sem, twin).wait_recv()

    def shared(mat, k, dy, dz):
        if mat:
            share(mat - 1, k, dy, dz).start()

    def pass_on(mat, dy, dz):
        k = 1 if home(dy, dz) else 0
        sized(
            short(core, group),
            lambda blocks: came(
                landing(mat, core, source(dy, dz, k), blocks), b_recv.at[mat, 2 * dz + dy]
            ),
        )
        if not k:
            relay(mat, dy, dz, lambda copy: copy.start())
        shared(mat, k, dy, dz)

    def pass_on_near(mat):
        pass_on(mat, 0, 0)
        pass_on(mat, 1, 0)

    def pass_on_from(mat, dy, zz):
        pass_on(mat, dy, (z + deep - zz) % deep)

    def passed(mat, *levels):
        def one(dy, dz):
            sized(
                short(core, group),
                lambda blocks: came(
                    landing(mat, core, source(dy, dz, 1), blocks), f_recv.at[mat, 2 * dz + dy]
                ),
            )
            shared(mat, 1, dy, dz)

        for zz in levels:
            if zz is None:
                one(1, 0)
            else:
                for dy in range(2):
                    one(dy, (z + deep - zz) % deep)

    def local(mat, run):
        def copy(blocks):
            run(
                pltpu.make_async_copy(
                    taken(mat, group, blocks), landing(mat, core, me, blocks), own_sem.at[mat]
                )
            )

        sized(short(core, group), copy)

    keep_proj = pltpu.make_async_copy(out_proj, proj, own_sem.at[3])

    last_block = (wide - 1) * LANES
    w1[core, :, last_block:span] = jnp.zeros((w1.shape[1], LANES), jnp.bfloat16)
    w1[core, :, span + last_block :] = jnp.zeros((w1.shape[1], LANES), jnp.bfloat16)
    tail = pl.ds(pl.multiple_of(core * span + last_block, LANES), LANES)
    w2[tail] = jnp.zeros((LANES, inner), jnp.bfloat16)

    with jax.named_scope("greet"):
        partners = [at(x, *target(dy, dz)) for dy, dz in sides[1:]]
        partners += [x_place, at(*fellow(3), z), twin]
        greet(partners)
    for zz in (inner_z, edge_z, pair):
        send_to(0, 0, zz)
    for mat in range(3):
        local(mat, lambda copy: copy.start())
    keep_proj.start()

    with jax.named_scope("local"):
        tokens = queries.shape[0]
        heads = queries.shape[1] // HK
        blocks = tokens // SPAN
        raw = decay_pre[...]
        logdecay = (jnp.minimum(raw, 0.0) - jnp.log1p(jnp.exp(-jnp.abs(raw)))) / TAU
        row = lax.broadcasted_iota(jnp.int32, (tokens, tokens), 0)
        col = lax.broadcasted_iota(jnp.int32, (tokens, tokens), 1)
        tri = jnp.logical_and(row // SPAN == col // SPAN, col <= row).astype(jnp.float32)
        cumul = jnp.dot(
            tri, logdecay, precision=lax.Precision.HIGHEST, preferred_element_type=jnp.float32
        )
        lasts = [cumul[(n + 1) * SPAN - 1 : (n + 1) * SPAN] for n in range(blocks)]
        across = (((0,), (0,)), ((), ()))

        def column(line):
            return jnp.broadcast_to(line, (HK, HK)).T

        def spread(square):
            return jnp.concatenate([square] * (HV // HK), axis=1)

        for n in range(blocks):
            steps = slice(n * SPAN, (n + 1) * SPAN)
            faded = keys[steps].astype(jnp.float32) * jnp.exp(lasts[n] - cumul[steps])
            high = faded.astype(jnp.bfloat16)
            low = (faded - high.astype(jnp.float32)).astype(jnp.bfloat16)
            for h in range(heads):
                key = slice(h * HK, (h + 1) * HK)
                value = values[steps, h * HV : (h + 1) * HV]
                updates[n, h] = lax.dot_general(
                    high[:, key], value, across, preferred_element_type=jnp.float32
                ) + lax.dot_general(
                    low[:, key], value, across, preferred_element_type=jnp.float32
                )
                ends[n, h] = column(jnp.exp(lasts[n][:, key]))
        whole = jnp.exp(sum(lasts))
        for h in range(heads):
            state = updates[0, h]
            for n in range(1, blocks):
                state = spread(ends[n, h]) * state + updates[n, h]
            s_out[h] = state.astype(jnp.bfloat16)
            d_out[h] = jnp.broadcast_to(whole[:, h * HK : (h + 1) * HK], d_out.shape[1:])

    def to_plane(dp):
        xx, yy = fellow(dp)
        goal, slot = at(xx, yy, z), 2 * yy + xx
        return (
            remote(s_out.at[slot], s_in.at[place], p1_send.at[dp, 0], p1_recv.at[dp, 0], goal),
            remote(d_out.at[slot], d_in.at[place], p1_send.at[dp, 1], p1_recv.at[dp, 1], goal),
        )

    for dp in range(1, plane):
        for copy in to_plane(dp):
            copy.start()
    s_in[place] = s_out[place]
    d_in[place] = d_out[place]
    send_near(0)

    with jax.named_scope("p1"):
        for dp in range(1, plane):
            for copy in to_plane(dp):
                copy.wait_recv()
    running = jnp.zeros((HK, HV), jnp.float32)
    line = jnp.ones((1, HK), jnp.float32)
    reach = []
    for i in range(plane):
        before[i] = running
        reach.append(line)
        own_decay = d_in[i][:1]
        running = spread(column(own_decay)) * running + s_in[i].astype(jnp.float32)
        line = line * own_decay
    total[...] = jnp.zeros(total.shape, jnp.float32)

    def to_next():
        return remote(t_out, t_in, p2_sem.at[0], p2_sem.at[1], above)

    def push_on():
        t_out[...] = (spread(column(line)) * total[...] + running).astype(jnp.bfloat16)
        to_next().start()

    @pl.when(z == 0)
    def _():
        push_on()

    @pl.when(jnp.logical_not(bottom))
    def _():
        for mat, dy, zz in ((1, 0, inner_z), (1, 0, edge_z), (0, 1, inner_z)):
            send_to(mat, dy, zz)

    with jax.named_scope("p2"):

        @pl.when(z > 0)
        def _():
            came(t_in, p2_sem.at[1])
            total[...] = t_in[...].astype(jnp.float32)

    @pl.when(jnp.logical_and(z > 0, z < deep - 1))
    def _():
        push_on()

    for i in range(plane):
        s_start[i] = (before[i] + spread(column(reach[i])) * total[...]).astype(jnp.bfloat16)

    def to_fellow(dp):
        xx, yy = fellow(dp)
        slot = 2 * yy + xx
        return remote(
            s_start.at[slot], start.at[place], p3_send.at[dp], p3_recv.at[dp], at(xx, yy, z)
        )

    for dp in range(1, plane):
        to_fellow(dp).start()
    start[place] = s_start[place]
    send_to(1, 0, pair)
    send_to(2, 0, pair)
    send_to(0, 1, pair)

    @pl.when(bottom)
    def _():
        for zz in (inner_z, edge_z):
            send_to(1, 0, zz)
            send_to(0, 1, zz)

    @pl.when(jnp.logical_not(bottom))
    def _():
        send_to(0, 1, edge_z)

    send_near(1)
    send_near(2)
    with jax.named_scope("gates2"):
        pass_on_near(0)
        for zz in (pair, edge_z, inner_z):
            pass_on_from(0, 0, zz)
    with jax.named_scope("p3"):
        for dp in range(1, plane):
            to_fellow(dp).wait_recv()

    with jax.named_scope("mix"):
        for h in range(heads):
            thick = slice(h * HV, (h + 1) * HV)
            state = start[h].astype(jnp.float32)
            reads = []
            for n in range(blocks):
                state = spread(ends[n, h]) * state + updates[n, h]
                high = state.astype(jnp.bfloat16)
                low = (state - high.astype(jnp.float32)).astype(jnp.bfloat16)
                query = queries[n * SPAN : (n + 1) * SPAN, h * HK : (h + 1) * HK]
                reads.append(
                    jnp.dot(query, high, preferred_element_type=jnp.float32)
                    + jnp.dot(query, low, preferred_element_type=jnp.float32)
                )
            read = jnp.concatenate(reads, axis=0) * HK ** (-0.5)
            size = jnp.mean(read * read, axis=-1, keepdims=True)
            pre = out_gate[:, thick].astype(jnp.float32)
            normed = read * lax.rsqrt(size + RMS_EPS) * head_gain[...]
            gated[:, thick] = (normed * (pre * jax.nn.sigmoid(pre))).astype(jnp.bfloat16)
    keep_proj.wait()
    with jax.named_scope("proj"):
        summed_heads = jnp.dot(gated[...], proj[...], preferred_element_type=jnp.float32)
        mixed[...] = summed_heads.astype(jnp.bfloat16).reshape(2, own, inner)
    swap = remote(mixed.at[1 - core], mixed_in, m_sem.at[0], m_sem.at[1], twin)
    swap.start()
    with jax.named_scope("swap"):
        swap.wait()
    with jax.named_scope("ln"):
        added = mixed[core].astype(jnp.float32) + mixed_in[...].astype(jnp.float32)
        middle = ALPHA * resid[core].astype(jnp.float32) + added
        rows[y, z] = layer_norm(middle, mix_gain[...], mix_shift[...]).astype(jnp.bfloat16)

    halves = range(2)
    chunk = own // 2
    bit = [pl.ds(h * chunk, chunk) for h in halves]

    def climb(zz, h):
        block = rows.at[y, zz, bit[h]]
        return remote(block, block, au_send.at[zz, h], az_recv.at[zz, h], above)

    def sink(zz, h):
        block = rows.at[y, zz, bit[h]]
        return remote(block, block, av_send.at[zz, h], az_recv.at[zz, h], below)

    def cross_y(zz, h):
        block = rows.at[y, zz, bit[h]]
        return remote(block, block, ay_send.at[zz, h], ay_recv.at[zz, h], y_place)

    for h in halves:

        @pl.when(z < deep - 1)
        def _():
            climb(z, h).start()

        @pl.when(z > 0)
        def _():
            sink(z, h).start()

        cross_y(z, h).start()

    def landed(far):
        for h in halves:

            @pl.when(z >= far)
            def _():
                came(rows.at[y, z - far, bit[h]], az_recv.at[z - far, h])

                @pl.when(z < deep - 1)
                def _():
                    climb(z - far, h).start()

                cross_y(z - far, h).start()

            @pl.when(z < deep - far)
            def _():
                came(rows.at[y, z + far, bit[h]], az_recv.at[z + far, h])

                @pl.when(z > 0)
                def _():
                    sink(z + far, h).start()

                cross_y(z + far, h).start()

    with jax.named_scope("wa"):
        for mat in range(3):
            local(mat, lambda copy: copy.wait())
        share(0, 0, 0, 0).start()
        share(1, 0, 0, 0).start()
        pass_on_near(1)
        for zz in (pair, edge_z, inner_z):
            pass_on_from(1, 0, zz)
        pass_on_from(0, 1, pair)
        pass_on_from(2, 0, pair)
    with jax.named_scope("ag1"):
        landed(1)

    send_to(1, 1, pair)
    send_to(2, 1, pair)

    def second_wave():
        for zz in (inner_z, edge_z):
            send_to(1, 1, zz)
        for dy in range(2):
            for zz in (inner_z, edge_z):
                send_to(2, dy, zz)

    @pl.when(jnp.logical_not(edge))
    def _():
        second_wave()

    with jax.named_scope("wb"):
        for zz in (edge_z, inner_z):
            pass_on_from(0, 1, zz)
        pass_on_near(2)
    with jax.named_scope("ag2"):
        landed(2)

    @pl.when(jnp.logical_not(edge))
    def _():
        pl.semaphore_signal(
            go_sem, inc=1, device_id=at(x, y, edge_z), device_id_type=MESH
        )

    with jax.named_scope("go"):

        @pl.when(edge)
        def _():
            pl.semaphore_wait(go_sem, 1)
            second_wave()

    with jax.named_scope("wc"):
        pass_on_from(1, 1, pair)
    with jax.named_scope("ag3"):
        for far in range(3, deep):
            landed(far)
    with jax.named_scope("wd"):
        pass_on_from(1, 1, inner_z)
        pass_on_from(1, 1, edge_z)
        pass_on_from(2, 1, pair)
        pass_on_from(2, 0, edge_z)
        pass_on_from(2, 0, inner_z)
    with jax.named_scope("we"):
        pass_on_from(2, 1, edge_z)
        pass_on_from(2, 1, inner_z)
    with jax.named_scope("wf"):
        passed(0, None, pair, edge_z, inner_z)
        passed(1, None, pair, edge_z, inner_z)
    with jax.named_scope("agy"):
        for zz in range(deep):
            for h in halves:
                came(rows.at[1 - y, zz, bit[h]], ay_recv.at[zz, h])
    def twins(j, *levels):
        for zz in levels:
            dz = 0 if zz is None else (z + deep - zz) % deep
            for k in range(2):
                for dy in range(2):
                    came(slab(j, 1 - core, source(dy, dz, k)), t_recv.at[j, k, 2 * dz + dy])

    with jax.named_scope("wt"):
        twins(0, None, pair, edge_z, inner_z)

    def hide(side, slot):
        left = rows[side].reshape(deep * own, inner)
        for c in range(2):
            both = jnp.dot(left, w1[c], preferred_element_type=jnp.float32)
            gate, up = both[:, :span], both[:, span:]
            hidden[slot, :, c * span : (c + 1) * span] = (
                gate * jax.nn.sigmoid(gate) * up
            ).astype(jnp.bfloat16)

    wing = inner // 2
    early = jnp.where(bottom, 0, 1)
    late = 1 - early
    columns = lambda h: pl.ds(pl.multiple_of(h * wing, wing), wing)

    def lower(side, slot, h):
        down = jnp.dot(hidden[slot], w2[:, columns(h)], preferred_element_type=jnp.float32)
        part[side, :, :, columns(h)] = down.astype(jnp.bfloat16).reshape(deep, own, wing)

    order = [
        jnp.where(bottom, deep - 1, 0),
        jnp.where(bottom, deep - 2, 1),
        jnp.where(bottom, 1 - z, 2 * deep - 3 - z),
        z,
    ]

    def across_y(d, h):
        return remote(
            part.at[1 - y, d, :, columns(h)],
            y_in.at[d, :, columns(h)],
            ry_send.at[d, h],
            ry_recv.at[d, h],
            y_place,
        )

    def hop(i, h, up):
        into, sem = (u_in, ru_recv) if up else (v_in, rv_recv)
        return remote(
            z_out.at[i, :, columns(h)],
            into.at[order[i], :, columns(h)],
            rz_send.at[i, h],
            sem.at[order[i], h],
            above if up else below,
        )

    def gather_in(d, h, from_below, from_above):
        taken = columns(h)
        came(y_in.at[d, :, taken], ry_recv.at[d, h])
        acc[:, taken] = part[y, d, :, taken].astype(jnp.float32) + y_in[d, :, taken].astype(
            jnp.float32
        )

        @pl.when(from_below)
        def _():
            came(u_in.at[d, :, taken], ru_recv.at[d, h])
            acc[:, taken] += u_in[d, :, taken].astype(jnp.float32)

        @pl.when(from_above)
        def _():
            came(v_in.at[d, :, taken], rv_recv.at[d, h])
            acc[:, taken] += v_in[d, :, taken].astype(jnp.float32)

    def step(i, h):
        d = order[i]
        up = d > z
        gather_in(
            d,
            h,
            jnp.logical_and(up, z > 0),
            jnp.logical_and(jnp.logical_not(up), z < deep - 1),
        )
        z_out[i, :, columns(h)] = acc[:, columns(h)].astype(jnp.bfloat16)

        @pl.when(up)
        def _():
            hop(i, h, True).start()

        @pl.when(jnp.logical_not(up))
        def _():
            hop(i, h, False).start()

    with jax.named_scope("hide0"):
        hide(1 - y, 0)
    with jax.named_scope("wg"):
        passed(2, None, pair)
        twins(1, None, pair)
    with jax.named_scope("down0"):
        lower(1 - y, 0, early)
    for d in order[:2]:
        across_y(d, early).start()
    with jax.named_scope("hide1"):
        hide(y, 1)
    with jax.named_scope("down1"):
        lower(y, 1, early)
    with jax.named_scope("wh"):
        passed(2, edge_z, inner_z)
        twins(1, edge_z, inner_z)
    with jax.named_scope("down2"):
        lower(1 - y, 0, late)
    for d in order[:2]:
        across_y(d, late).start()
    for d in order[2:]:
        for h in (early, late):
            across_y(d, h).start()
    with jax.named_scope("down3"):
        lower(y, 1, late)
    for i, h in ((0, early), (1, early), (0, late), (1, late), (2, early), (2, late)):
        with jax.named_scope("rs%d%d" % (i, h is late)):
            step(i, h)
    with jax.named_scope("rsend0"):
        gather_in(z, early, z > 0, z < deep - 1)
    with jax.named_scope("rsend1"):
        gather_in(z, late, z > 0, z < deep - 1)
    with jax.named_scope("fin"):
        finished = layer_norm(
            ALPHA * rows[y, z].astype(jnp.float32) + 0.5 * acc[...], gain[...], shift[...]
        )
        out[core] = finished.astype(jnp.bfloat16)
    last = remote(out.at[core], out.at[core], f_sem.at[0, 0], f_sem.at[1, 0], twin)
    last.start()

    with jax.named_scope("drain"):

        @pl.when(z < deep - 1)
        def _():
            to_next().wait_send()

        for dy, dz in sides:
            for mat in range(3):
                bring(mat, dy, dz, lambda copy: copy.wait_send())
                if (dy, dz) != (0, 0):
                    relay(mat, dy, dz, lambda copy: copy.wait_send())
            for j in range(2):
                for k in range(2):
                    share(j, k, dy, dz).wait_send()
        for dp in range(1, plane):
            for copy in (*to_plane(dp), to_fellow(dp)):
                copy.wait_send()
        for zz in range(deep):

            for h in halves:

                @pl.when(jnp.logical_and(zz <= z, z < deep - 1))
                def _():
                    climb(zz, h).wait_send()

                @pl.when(jnp.logical_and(zz >= z, z > 0))
                def _():
                    sink(zz, h).wait_send()

                cross_y(zz, h).wait_send()
                across_y(zz, h).wait_send()
        for h in halves:
            for i in range(deep - 1):
                hop(i, h, True).wait_send()
        last.wait()


def layer(
    resid,
    queries,
    keys,
    values,
    decay_pre,
    out_gate,
    head_gain,
    out_proj,
    mix_gain,
    mix_shift,
    gate_in,
    up_in,
    down_out,
    gain,
    shift,
):
    count = lax.axis_size("sp")
    tok_rows, inner = resid.shape
    own = tok_rows // 2
    deep = count // 4
    groups = count // 2
    wide = -(-(gate_in.shape[1] // LANES) // groups)
    span = wide * LANES
    heads = queries.shape[1] // HK
    steps = tok_rows // SPAN
    dma = pltpu.SemaphoreType.DMA
    half, full = jnp.bfloat16, jnp.float32
    block = lambda *lead: pltpu.VMEM((*lead, own, inner), half)
    near, far = pl.BlockSpec(memory_space=pltpu.VMEM), pl.BlockSpec(memory_space=pl.ANY)
    out = pl.pallas_call(
        functools.partial(layer_kernel, deep, wide),
        out_shape=jax.ShapeDtypeStruct((2, own, inner), half),
        in_specs=[near] * 6 + [far] + [near] * 3 + [far] * 3 + [near] * 2,
        out_specs=near,
        scratch_shapes=[
            pltpu.VMEM((2, inner, 2 * span), half),
            pltpu.VMEM((2 * span, inner), half),
            pltpu.VMEM(out_proj.shape, half),
            pltpu.VMEM((steps, heads, HK, HV), full),
            pltpu.VMEM((steps, heads, HK, HK), full),
            pltpu.VMEM((heads, HK, HV), half),
            pltpu.VMEM((heads, 8, HK), full),
            pltpu.VMEM((4, HK, HV), half),
            pltpu.VMEM((4, 8, HK), full),
            pltpu.VMEM((4, HK, HV), full),
            pltpu.VMEM((HK, HV), full),
            pltpu.VMEM((HK, HV), half),
            pltpu.VMEM((HK, HV), half),
            pltpu.VMEM((4, HK, HV), half),
            pltpu.VMEM((4, HK, HV), half),
            pltpu.VMEM((tok_rows, out_proj.shape[0]), half),
            block(2),
            block(),
            block(2, deep),
            pltpu.VMEM((2, deep * own, 2 * span), half),
            block(2, deep),
            block(deep),
            block(deep),
            block(deep),
            block(deep - 1),
            pltpu.VMEM((own, inner), full),
            dma((4,)),
            dma((3, groups)),
            dma((3, groups)),
            dma((3, groups)),
            dma((3, groups)),
            dma((2, 2, groups)),
            dma((2, 2, groups)),
            dma((4, 2)),
            dma((4, 2)),
            dma((2,)),
            dma((4,)),
            dma((4,)),
            dma((2,)),
            *[dma((deep, 2))] * 10,
            dma((2, 2)),
            pltpu.SemaphoreType.REGULAR,
        ],
        compiler_params=pltpu.CompilerParams(
            collective_id=2, has_side_effects=True, vmem_limit_bytes=60 * 1024 * 1024
        ),
    )(
        queries,
        keys,
        values,
        decay_pre,
        out_gate,
        head_gain[None],
        out_proj,
        resid.reshape(2, own, inner),
        mix_gain[None],
        mix_shift[None],
        gate_in,
        up_in,
        down_out,
        gain[None],
        shift[None],
    )
    return out.reshape(tok_rows, inner)


def body(
    resid,
    queries,
    keys,
    values,
    decay_pre,
    out_gate,
    head_gain,
    out_proj,
    mix_gain,
    mix_shift,
    gate_in,
    up_in,
    down_out,
    out_gain,
    out_shift,
):
    tp_count = lax.axis_size("tp")
    tok_rows = queries.shape[0]
    own_count = tok_rows // tp_count
    sp_count = lax.axis_size("sp")
    units = gate_in.shape[1]
    heads = queries.shape[1] // HK
    groups = sp_count // 2
    unit_blocks = units // LANES
    by_units = (
        tp_count == 2
        and sp_count == 16
        and heads == 4
        and units % LANES == 0
        and unit_blocks % groups == groups - 2
        and gate_in.shape[0] % LANES == 0
        and down_out.shape[1] % LANES == 0
        and gate_in.shape[0] * sp_count == resid.shape[1]
        and own_count % 16 == 0
        and tok_rows % SPAN == 0
    )
    if by_units:
        return layer(
            resid,
            queries,
            keys,
            values,
            decay_pre,
            out_gate,
            head_gain,
            out_proj,
            mix_gain,
            mix_shift,
            gate_in,
            up_in,
            down_out,
            out_gain,
            out_shift,
        )
    local = local_tokens(queries, keys, values, decay_pre)
    gated = mix_tokens(*local, out_gate, head_gain)
    mixed = lax.psum_scatter(
        jnp.dot(gated, out_proj, preferred_element_type=jnp.float32).astype(jnp.bfloat16),
        "tp",
        scatter_dimension=0,
        tiled=True,
    ).astype(jnp.float32)
    own_resid = lax.dynamic_slice_in_dim(resid, lax.axis_index("tp") * own_count, own_count, 0)
    mid = layer_norm(ALPHA * own_resid.astype(jnp.float32) + mixed, mix_gain, mix_shift).astype(
        jnp.bfloat16
    )
    whole_rows = lax.all_gather(mid, "tp", axis=0, tiled=True)
    hidden = hidden_by_rows(whole_rows, gate_in, up_in)
    ffn = lax.psum_scatter(
        down_by_columns(hidden, down_out).astype(jnp.bfloat16),
        "tp",
        scatter_dimension=0,
        tiled=True,
    ).astype(jnp.float32)
    finished = layer_norm(ALPHA * mid.astype(jnp.float32) + 0.5 * ffn, out_gain, out_shift).astype(
        jnp.bfloat16
    )
    return lax.all_gather(finished, "tp", axis=0, tiled=True)


def solution(mesh):
    return jax.shard_map(
        body,
        mesh=mesh,
        in_specs=(
            P("sp", None),
            P("sp", "tp"),
            P("sp", "tp"),
            P("sp", "tp"),
            P("sp", "tp"),
            P("sp", "tp"),
            P(),
            P("tp", None),
            P(),
            P(),
            P("sp", "tp"),
            P("sp", "tp"),
            P("tp", "sp"),
            P(),
            P(),
        ),
        out_specs=P("sp", None),
        check_vma=False,
    )
```

```python
import functools

import jax
import jax.numpy as jnp
from jax import lax
from jax.experimental import pallas as pl
from jax.experimental.pallas import tpu as pltpu
from jax.sharding import PartitionSpec as P

HK = 128
HV = 256
SPAN = 64
LANES = 128


ALPHA = 2.0**0.25
LN_EPS = 1e-05
RMS_EPS = 1e-06
TAU = 16.0
MESH = pl.DeviceIdType.MESH


def entering(array, axis, combine, identity):
    count, place = (lax.axis_size(axis), lax.axis_index(axis))
    everything = jax.tree.map(
        lambda part, kind: lax.all_gather(part.astype(kind), axis),
        array,
        (jnp.bfloat16, jnp.bfloat16),
    )
    start = jax.tree.map(
        lambda part, zero: jnp.broadcast_to(jnp.asarray(zero, part.dtype), part.shape),
        array,
        identity,
    )

    def lap(k, before):
        reached = k < place
        new = combine(
            before, jax.tree.map(lambda part, own: part[k].astype(own.dtype), everything, array)
        )
        return jax.tree.map(lambda a, b: jnp.where(reached, a, b), new, before)

    return lax.fori_loop(0, count, lap, start)


def layer_norm(inputs, gain, shift):
    center = inputs - jnp.mean(inputs, axis=-1, keepdims=True)
    spread = jnp.mean(center * center, axis=-1, keepdims=True)
    return center * lax.rsqrt(spread + LN_EPS) * gain + shift


def combine_states(earlier, later):
    return (earlier[0] * later[0], later[0][..., None] * earlier[1] + later[1])


def greet(places):
    barrier = pltpu.get_barrier_semaphore()
    for place in places:
        pl.semaphore_signal(barrier, inc=1, device_id=place, device_id_type=MESH)
    pl.semaphore_wait(barrier, len(places))


def remote(src, dst, send, recv, place):
    return pltpu.make_async_remote_copy(
        src_ref=src, dst_ref=dst, send_sem=send, recv_sem=recv, device_id=place, device_id_type=MESH
    )


def local_tokens(queries, keys, values, decay_pre):
    tok_rows = queries.shape[0]
    local_heads = queries.shape[1] // HK
    blocks = tok_rows // SPAN
    logdecay = jax.nn.log_sigmoid(decay_pre) / TAU
    scaled_q = queries.astype(jnp.float32).reshape(blocks, SPAN, local_heads, HK) * HK ** (-0.5)
    key_block = keys.astype(jnp.float32).reshape(blocks, SPAN, local_heads, HK)
    value_block = values.astype(jnp.float32).reshape(blocks, SPAN, local_heads, HV)
    cumul = jnp.cumsum(logdecay.reshape(blocks, SPAN, local_heads, HK), axis=1)
    last = cumul[:, -1]
    key_decayed = key_block * jnp.exp(last[:, None] - cumul)
    updates = jnp.einsum(
        "nchk,nchv->nhkv", key_decayed, value_block, precision=lax.Precision.HIGHEST
    )

    def advance(running_state, inputs):
        decay_end, state_increment, current_query = inputs
        running_state = jnp.exp(decay_end)[..., None] * running_state + state_increment
        return (
            running_state,
            jnp.einsum(
                "qpy,pyr->qpr", current_query, running_state, precision=lax.Precision.HIGHEST
            ),
        )

    own_state, local_read = lax.scan(
        advance, jnp.zeros((local_heads, HK, HV), jnp.float32), (last, updates, scaled_q)
    )
    block_ends = jnp.cumsum(last, axis=0)
    own_decay = jnp.exp(block_ends[-1])
    carry_q = scaled_q * jnp.exp(block_ends)[:, None]
    return local_read, carry_q, own_decay, own_state


def mix_tokens(local_read, carry_q, own_decay, own_state, out_gate, head_gain):
    blocks, span, local_heads, _ = carry_q.shape
    tok_rows = blocks * span
    identity = (jnp.ones_like(own_decay), jnp.zeros_like(own_state))
    _, incoming = entering((own_decay, own_state), "sp", combine_states, identity)
    carried = jnp.einsum(
        "xepj,pjw->xepw", carry_q, incoming, precision=lax.Precision.HIGHEST
    )
    state_readout = (local_read + carried).reshape(tok_rows, local_heads, HV)
    normed = (
        state_readout
        * lax.rsqrt(jnp.mean(state_readout * state_readout, axis=-1, keepdims=True) + RMS_EPS)
        * head_gain
    )
    return (
        normed.reshape(tok_rows, local_heads * HV) * jax.nn.silu(out_gate.astype(jnp.float32))
    ).astype(jnp.bfloat16)


def hidden_by_rows(whole_rows, gate_in, up_in):
    gate = jnp.dot(
        whole_rows,
        lax.all_gather(gate_in, "sp", axis=0, tiled=True),
        preferred_element_type=jnp.float32,
    )
    upward = jnp.dot(
        whole_rows,
        lax.all_gather(up_in, "sp", axis=0, tiled=True),
        preferred_element_type=jnp.float32,
    )
    return (jax.nn.silu(gate) * upward).astype(jnp.bfloat16)


def down_by_columns(hidden, down_out):
    return jnp.dot(
        hidden,
        lax.all_gather(down_out, "sp", axis=1, tiled=True),
        preferred_element_type=jnp.float32,
    )


def layer_kernel(
    deep,
    wide,
    queries_far,
    keys_far,
    values_far,
    decay_pre_far,
    out_gate_far,
    head_gain,
    out_proj,
    resid_far,
    mix_gain,
    mix_shift,
    gate_in,
    up_in,
    down_out,
    gain,
    shift,
    out,
    queries,
    keys,
    values,
    decay_pre,
    out_gate,
    resid,
    w1,
    w2,
    proj,
    updates,
    ends,
    s_out,
    d_out,
    s_in,
    d_in,
    before,
    total,
    t_out,
    t_in,
    s_start,
    start,
    gated,
    mixed,
    mixed_in,
    rows,
    hidden,
    part,
    y_in,
    u_in,
    v_in,
    z_out,
    acc,
    own_sem,
    b_send,
    b_recv,
    f_send,
    f_recv,
    t_send,
    t_recv,
    p1_send,
    p1_recv,
    p2_sem,
    p3_send,
    p3_recv,
    m_sem,
    au_send,
    av_send,
    ay_send,
    az_recv,
    ay_recv,
    ry_send,
    ry_recv,
    rz_send,
    ru_recv,
    rv_recv,
    f_sem,
    go_sem,
    near_sem,
):
    me, core = lax.axis_index("sp"), lax.axis_index("tp")
    x, y, z = me % 2, (me // 2) % 2, me // 4
    group = me // 2
    groups = 2 * deep
    plane = 4
    place = me % plane
    own, inner = rows.shape[2], rows.shape[3]
    depth = gate_in.shape[0]
    lanes = down_out.shape[1]
    span = wide * LANES
    half = lambda c: pl.ds(pl.multiple_of(c * span, span), span)
    twin = (me, 1 - core)
    x_place = (me + 1 - 2 * x, core)
    y_place = (me + 2 - 4 * y, core)
    above, below = (me + plane, core), (me - plane, core)
    sides = [(dy, dz) for dz in range(deep) for dy in range(2)]
    bottom = z < deep // 2
    edge = jnp.logical_or(z == 0, z == deep - 1)
    pair = z + 1 - 2 * (z % 2)
    inner_z = jnp.where(bottom, deep // 2, deep // 2 - 1)
    edge_z = jnp.where(bottom, deep - 1, 0)

    def at(xx, yy, zz):
        return (plane * zz + 2 * yy + xx, core)

    def target(dy, dz):
        return (y + dy) % 2, (z + dz) % deep

    def origin(dy, dz):
        return (y + dy) % 2, (z + deep - dz) % deep

    def fellow(dp):
        return (x + dp % 2) % 2, (y + dp // 2) % 2

    def short(c, g):
        return jnp.logical_or(g == c, g == groups - 2 + c)

    def first_block(c, g):
        return wide * g - (g > c).astype(jnp.int32) - (g > groups - 2 + c).astype(jnp.int32)

    def sized(flag, run):
        @pl.when(flag)
        def _():
            run(wide - 1)

        @pl.when(jnp.logical_not(flag))
        def _():
            run(wide)

    def taken(mat, g, blocks):
        begin = pl.ds(pl.multiple_of(first_block(core, g) * LANES, LANES), blocks * LANES)
        return (gate_in.at[:, begin], up_in.at[:, begin], down_out.at[begin])[mat]

    def landing(mat, c, s, blocks):
        if mat < 2:
            rows_of = pl.ds(pl.multiple_of(s * depth, depth), depth)
            return w1.at[c, rows_of, pl.ds(mat * span, blocks * LANES)]
        columns = pl.ds(pl.multiple_of(s * lanes, lanes), lanes)
        return w2.at[pl.ds(pl.multiple_of(c * span, span), blocks * LANES), columns]

    def slab(j, c, s):
        if j == 0:
            return w1.at[c, pl.ds(pl.multiple_of(s * depth, depth), depth)]
        return landing(2, c, s, wide)

    def home(dy, dz):
        return isinstance(dz, int) and dy == 0 and dz == 0

    def bring(mat, dy, dz, run):
        yy, zz = target(dy, dz)
        goal = x_place if home(dy, dz) else at(x, yy, zz)
        g = 2 * zz + yy
        r = 2 * dz + dy

        def copy(blocks):
            run(
                remote(
                    taken(mat, g, blocks),
                    landing(mat, core, me, blocks),
                    b_send.at[mat, r],
                    b_recv.at[mat, r],
                    goal,
                )
            )

        sized(short(core, g), copy)

    def send(mat, dy, dz):
        bring(mat, dy, dz, lambda copy: copy.start())

    def send_near(mat):
        send(mat, 0, 0)
        send(mat, 1, 0)

    def send_to(mat, dy, zz):
        send(mat, dy, (zz + deep - z) % deep)

    def source(dy, dz, k):
        yy, zz = origin(dy, dz)
        return plane * zz + 2 * yy + (x + k) % 2

    def relay(mat, dy, dz, run):
        r = 2 * dz + dy

        def copy(blocks):
            block = landing(mat, core, source(dy, dz, 0), blocks)
            run(remote(block, block, f_send.at[mat, r], f_recv.at[mat, r], x_place))

        sized(short(core, group), copy)

    def share(j, k, dy, dz):
        block = slab(j, core, source(dy, dz, k))
        r = 2 * dz + dy
        return remote(block, block, t_send.at[j, k, r], t_recv.at[j, k, r], twin)

    def came(ref, sem):
        remote(ref, ref, f_sem.at[0, 0], sem, twin).wait_recv()

    def shared(mat, k, dy, dz):
        if mat:
            share(mat - 1, k, dy, dz).start()

    def pass_on(mat, dy, dz):
        k = 1 if home(dy, dz) else 0
        sized(
            short(core, group),
            lambda blocks: came(
                landing(mat, core, source(dy, dz, k), blocks), b_recv.at[mat, 2 * dz + dy]
            ),
        )
        if not k:
            relay(mat, dy, dz, lambda copy: copy.start())
        shared(mat, k, dy, dz)

    def pass_on_near(mat):
        pass_on(mat, 0, 0)
        pass_on(mat, 1, 0)

    def pass_on_from(mat, dy, zz):
        pass_on(mat, dy, (z + deep - zz) % deep)

    def passed(mat, *levels):
        def one(dy, dz):
            sized(
                short(core, group),
                lambda blocks: came(
                    landing(mat, core, source(dy, dz, 1), blocks), f_recv.at[mat, 2 * dz + dy]
                ),
            )
            shared(mat, 1, dy, dz)

        for zz in levels:
            if zz is None:
                one(1, 0)
            else:
                for dy in range(2):
                    one(dy, (z + deep - zz) % deep)

    def local(mat, run):
        def copy(blocks):
            run(
                pltpu.make_async_copy(
                    taken(mat, group, blocks), landing(mat, core, me, blocks), own_sem.at[mat]
                )
            )

        sized(short(core, group), copy)

    keep_proj = pltpu.make_async_copy(out_proj, proj, own_sem.at[3])

    keep_near = [
        pltpu.make_async_copy(ref, copy, near_sem.at[i])
        for i, (ref, copy) in enumerate(
            (
                (decay_pre_far, decay_pre),
                (keys_far, keys),
                (values_far, values),
                (queries_far, queries),
                (out_gate_far, out_gate),
                (resid_far, resid),
            )
        )
    ]
    for copy in keep_near:
        copy.start()

    with jax.named_scope("greet"):
        partners = [at(x, *target(dy, dz)) for dy, dz in sides[1:]]
        partners += [x_place, at(*fellow(3), z), twin]
        greet(partners)
    for zz in (inner_z, edge_z, pair):
        send_to(0, 0, zz)
    for mat in range(3):
        local(mat, lambda copy: copy.start())
    keep_proj.start()

    with jax.named_scope("local"):
        for copy in keep_near[:3]:
            copy.wait()
        tokens = queries.shape[0]
        heads = queries.shape[1] // HK
        blocks = tokens // SPAN
        raw = decay_pre[...]
        logdecay = (jnp.minimum(raw, 0.0) - jnp.log1p(jnp.exp(-jnp.abs(raw)))) / TAU
        row = lax.broadcasted_iota(jnp.int32, (tokens, tokens), 0)
        col = lax.broadcasted_iota(jnp.int32, (tokens, tokens), 1)
        tri = jnp.logical_and(row // SPAN == col // SPAN, col <= row).astype(jnp.float32)
        cumul = jnp.dot(
            tri, logdecay, precision=lax.Precision.HIGHEST, preferred_element_type=jnp.float32
        )
        lasts = [cumul[(n + 1) * SPAN - 1 : (n + 1) * SPAN] for n in range(blocks)]
        across = (((0,), (0,)), ((), ()))

        def column(line):
            return jnp.broadcast_to(line, (HK, HK)).T

        def spread(square):
            return jnp.concatenate([square] * (HV // HK), axis=1)

        for n in range(blocks):
            steps = slice(n * SPAN, (n + 1) * SPAN)
            faded = keys[steps].astype(jnp.float32) * jnp.exp(lasts[n] - cumul[steps])
            high = faded.astype(jnp.bfloat16)
            low = (faded - high.astype(jnp.float32)).astype(jnp.bfloat16)
            for h in range(heads):
                key = slice(h * HK, (h + 1) * HK)
                value = values[steps, h * HV : (h + 1) * HV]
                updates[n, h] = lax.dot_general(
                    high[:, key], value, across, preferred_element_type=jnp.float32
                ) + lax.dot_general(
                    low[:, key], value, across, preferred_element_type=jnp.float32
                )
                ends[n, h] = column(jnp.exp(lasts[n][:, key]))
        whole = jnp.exp(sum(lasts))
        for h in range(heads):
            state = updates[0, h]
            for n in range(1, blocks):
                state = spread(ends[n, h]) * state + updates[n, h]
            s_out[h] = state.astype(jnp.bfloat16)
            d_out[h] = jnp.broadcast_to(whole[:, h * HK : (h + 1) * HK], d_out.shape[1:])

    def to_plane(dp):
        xx, yy = fellow(dp)
        goal, slot = at(xx, yy, z), 2 * yy + xx
        return (
            remote(s_out.at[slot], s_in.at[place], p1_send.at[dp, 0], p1_recv.at[dp, 0], goal),
            remote(d_out.at[slot], d_in.at[place], p1_send.at[dp, 1], p1_recv.at[dp, 1], goal),
        )

    for dp in range(1, plane):
        for copy in to_plane(dp):
            copy.start()
    s_in[place] = s_out[place]
    d_in[place] = d_out[place]
    send_near(0)

    @pl.when(short(core, group))
    def _():
        last_block = (wide - 1) * LANES
        blank = jnp.zeros((w1.shape[1], LANES), jnp.bfloat16)
        w1[core, :, last_block:span] = blank
        w1[core, :, span + last_block :] = blank
        tail = pl.ds(pl.multiple_of(core * span + last_block, LANES), LANES)
        w2[tail] = jnp.zeros((LANES, inner), jnp.bfloat16)

    with jax.named_scope("p1"):
        for dp in range(1, plane):
            for copy in to_plane(dp):
                copy.wait_recv()
    running = jnp.zeros((HK, HV), jnp.float32)
    line = jnp.ones((1, HK), jnp.float32)
    reach = []
    for i in range(plane):
        before[i] = running
        reach.append(line)
        own_decay = d_in[i][:1]
        running = spread(column(own_decay)) * running + s_in[i].astype(jnp.float32)
        line = line * own_decay
    total[...] = jnp.zeros(total.shape, jnp.float32)

    def to_next():
        return remote(t_out, t_in, p2_sem.at[0], p2_sem.at[1], above)

    def push_on():
        t_out[...] = (spread(column(line)) * total[...] + running).astype(jnp.bfloat16)
        to_next().start()

    @pl.when(z == 0)
    def _():
        push_on()

    @pl.when(jnp.logical_not(bottom))
    def _():
        for mat, dy, zz in ((1, 0, inner_z), (1, 0, edge_z), (0, 1, inner_z)):
            send_to(mat, dy, zz)

    def gates():
        pass_on_near(0)
        for zz in (pair, edge_z, inner_z):
            pass_on_from(0, 0, zz)

    with jax.named_scope("gates1"):

        @pl.when(jnp.logical_not(bottom))
        def _():
            gates()

    with jax.named_scope("p2"):

        @pl.when(z > 0)
        def _():
            came(t_in, p2_sem.at[1])
            total[...] = t_in[...].astype(jnp.float32)

    @pl.when(jnp.logical_and(z > 0, z < deep - 1))
    def _():
        push_on()

    for i in range(plane):
        s_start[i] = (before[i] + spread(column(reach[i])) * total[...]).astype(jnp.bfloat16)

    def to_fellow(dp):
        xx, yy = fellow(dp)
        slot = 2 * yy + xx
        return remote(
            s_start.at[slot], start.at[place], p3_send.at[dp], p3_recv.at[dp], at(xx, yy, z)
        )

    for dp in range(1, plane):
        to_fellow(dp).start()
    start[place] = s_start[place]
    send_to(1, 0, pair)
    send_to(2, 0, pair)
    send_to(0, 1, pair)

    @pl.when(bottom)
    def _():
        for zz in (inner_z, edge_z):
            send_to(1, 0, zz)
            send_to(0, 1, zz)

    @pl.when(jnp.logical_not(bottom))
    def _():
        send_to(0, 1, edge_z)

    send_near(1)
    send_near(2)
    with jax.named_scope("gates2"):

        @pl.when(bottom)
        def _():
            gates()

    with jax.named_scope("p3"):
        for dp in range(1, plane):
            to_fellow(dp).wait_recv()

    with jax.named_scope("mix"):
        for copy in keep_near[3:]:
            copy.wait()
        for h in range(heads):
            thick = slice(h * HV, (h + 1) * HV)
            state = start[h].astype(jnp.float32)
            reads = []
            for n in range(blocks):
                state = spread(ends[n, h]) * state + updates[n, h]
                high = state.astype(jnp.bfloat16)
                low = (state - high.astype(jnp.float32)).astype(jnp.bfloat16)
                query = queries[n * SPAN : (n + 1) * SPAN, h * HK : (h + 1) * HK]
                reads.append(
                    jnp.dot(query, high, preferred_element_type=jnp.float32)
                    + jnp.dot(query, low, preferred_element_type=jnp.float32)
                )
            read = jnp.concatenate(reads, axis=0) * HK ** (-0.5)
            size = jnp.mean(read * read, axis=-1, keepdims=True)
            pre = out_gate[:, thick].astype(jnp.float32)
            normed = read * lax.rsqrt(size + RMS_EPS) * head_gain[...]
            gated[:, thick] = (normed * (pre * jax.nn.sigmoid(pre))).astype(jnp.bfloat16)
    keep_proj.wait()
    with jax.named_scope("proj"):
        summed_heads = jnp.dot(gated[...], proj[...], preferred_element_type=jnp.float32)
        mixed[...] = summed_heads.astype(jnp.bfloat16).reshape(2, own, inner)
    swap = remote(mixed.at[1 - core], mixed_in, m_sem.at[0], m_sem.at[1], twin)
    swap.start()
    with jax.named_scope("swap"):
        swap.wait()
    with jax.named_scope("ln"):
        added = mixed[core].astype(jnp.float32) + mixed_in[...].astype(jnp.float32)
        middle = ALPHA * resid[core].astype(jnp.float32) + added
        rows[y, z] = layer_norm(middle, mix_gain[...], mix_shift[...]).astype(jnp.bfloat16)

    halves = range(2)
    chunk = own // 2
    bit = [pl.ds(h * chunk, chunk) for h in halves]

    def climb(zz, h):
        block = rows.at[y, zz, bit[h]]
        return remote(block, block, au_send.at[zz, h], az_recv.at[zz, h], above)

    def sink(zz, h):
        block = rows.at[y, zz, bit[h]]
        return remote(block, block, av_send.at[zz, h], az_recv.at[zz, h], below)

    def cross_y(zz, h):
        block = rows.at[y, zz, bit[h]]
        return remote(block, block, ay_send.at[zz, h], ay_recv.at[zz, h], y_place)

    for h in halves:

        @pl.when(z < deep - 1)
        def _():
            climb(z, h).start()

        @pl.when(z > 0)
        def _():
            sink(z, h).start()

        cross_y(z, h).start()

    ahead = jnp.logical_not(jnp.logical_or(bottom, edge))

    @pl.when(ahead)
    def _():
        for zz in (inner_z, edge_z):
            send_to(1, 1, zz)

    def landed(far):
        for h in halves:

            @pl.when(z >= far)
            def _():
                came(rows.at[y, z - far, bit[h]], az_recv.at[z - far, h])

                @pl.when(z < deep - 1)
                def _():
                    climb(z - far, h).start()

                cross_y(z - far, h).start()

            @pl.when(z < deep - far)
            def _():
                came(rows.at[y, z + far, bit[h]], az_recv.at[z + far, h])

                @pl.when(z > 0)
                def _():
                    sink(z + far, h).start()

                cross_y(z + far, h).start()

    with jax.named_scope("wa"):
        for mat in range(3):
            local(mat, lambda copy: copy.wait())
        share(0, 0, 0, 0).start()
        share(1, 0, 0, 0).start()
        pass_on_near(1)
        for zz in (pair, edge_z, inner_z):
            pass_on_from(1, 0, zz)
        pass_on_from(0, 1, pair)
        pass_on_from(2, 0, pair)
    with jax.named_scope("ag1"):
        landed(1)

    send_to(1, 1, pair)
    send_to(2, 1, pair)

    def second_wave():
        @pl.when(jnp.logical_not(ahead))
        def _():
            for zz in (inner_z, edge_z):
                send_to(1, 1, zz)

        for dy in range(2):
            for zz in (inner_z, edge_z):
                send_to(2, dy, zz)

    @pl.when(jnp.logical_not(edge))
    def _():
        second_wave()

    with jax.named_scope("wb"):
        for zz in (edge_z, inner_z):
            pass_on_from(0, 1, zz)
        pass_on_near(2)
    with jax.named_scope("ag2"):
        landed(2)

    @pl.when(jnp.logical_not(edge))
    def _():
        pl.semaphore_signal(
            go_sem, inc=1, device_id=at(x, y, edge_z), device_id_type=MESH
        )

    with jax.named_scope("go"):

        @pl.when(edge)
        def _():
            pl.semaphore_wait(go_sem, 1)
            second_wave()

    with jax.named_scope("wc"):
        pass_on_from(1, 1, pair)
    with jax.named_scope("ag3"):
        for far in range(3, deep):
            landed(far)
    with jax.named_scope("wd"):
        pass_on_from(1, 1, inner_z)
        pass_on_from(1, 1, edge_z)
        pass_on_from(2, 1, pair)
        pass_on_from(2, 0, edge_z)
        pass_on_from(2, 0, inner_z)
    with jax.named_scope("we"):
        pass_on_from(2, 1, edge_z)
        pass_on_from(2, 1, inner_z)
    with jax.named_scope("wf"):
        passed(0, None, pair, edge_z, inner_z)
        passed(1, None, pair, edge_z, inner_z)
    with jax.named_scope("agy"):
        for zz in range(deep):
            for h in halves:
                came(rows.at[1 - y, zz, bit[h]], ay_recv.at[zz, h])
    def twins(j, *levels):
        for zz in levels:
            dz = 0 if zz is None else (z + deep - zz) % deep
            for k in range(2):
                for dy in range(2):
                    came(slab(j, 1 - core, source(dy, dz, k)), t_recv.at[j, k, 2 * dz + dy])

    with jax.named_scope("wt"):
        twins(0, None, pair, edge_z, inner_z)

    def hide(side, slot):
        left = rows[side].reshape(deep * own, inner)
        for c in range(2):
            both = jnp.dot(left, w1[c], preferred_element_type=jnp.float32)
            gate, up = both[:, :span], both[:, span:]
            hidden[slot, :, c * span : (c + 1) * span] = (
                gate * jax.nn.sigmoid(gate) * up
            ).astype(jnp.bfloat16)

    wing = inner // 2
    early = jnp.where(bottom, 0, 1)
    late = 1 - early
    columns = lambda h: pl.ds(pl.multiple_of(h * wing, wing), wing)

    def lower(side, slot, h):
        down = jnp.dot(hidden[slot], w2[:, columns(h)], preferred_element_type=jnp.float32)
        part[side, :, :, columns(h)] = down.astype(jnp.bfloat16).reshape(deep, own, wing)

    order = [
        jnp.where(bottom, deep - 1, 0),
        jnp.where(bottom, deep - 2, 1),
        jnp.where(bottom, 1 - z, 2 * deep - 3 - z),
        z,
    ]

    def across_y(d, h):
        return remote(
            part.at[1 - y, d, :, columns(h)],
            y_in.at[d, :, columns(h)],
            ry_send.at[d, h],
            ry_recv.at[d, h],
            y_place,
        )

    def hop(i, h, up):
        into, sem = (u_in, ru_recv) if up else (v_in, rv_recv)
        return remote(
            z_out.at[i, :, columns(h)],
            into.at[order[i], :, columns(h)],
            rz_send.at[i, h],
            sem.at[order[i], h],
            above if up else below,
        )

    def gather_in(d, h, from_below, from_above):
        taken = columns(h)
        came(y_in.at[d, :, taken], ry_recv.at[d, h])
        acc[:, taken] = part[y, d, :, taken].astype(jnp.float32) + y_in[d, :, taken].astype(
            jnp.float32
        )

        @pl.when(from_below)
        def _():
            came(u_in.at[d, :, taken], ru_recv.at[d, h])
            acc[:, taken] += u_in[d, :, taken].astype(jnp.float32)

        @pl.when(from_above)
        def _():
            came(v_in.at[d, :, taken], rv_recv.at[d, h])
            acc[:, taken] += v_in[d, :, taken].astype(jnp.float32)

    def step(i, h):
        d = order[i]
        up = d > z
        gather_in(
            d,
            h,
            jnp.logical_and(up, z > 0),
            jnp.logical_and(jnp.logical_not(up), z < deep - 1),
        )
        z_out[i, :, columns(h)] = acc[:, columns(h)].astype(jnp.bfloat16)

        @pl.when(up)
        def _():
            hop(i, h, True).start()

        @pl.when(jnp.logical_not(up))
        def _():
            hop(i, h, False).start()

    with jax.named_scope("hide0"):
        hide(1 - y, 0)
    with jax.named_scope("wg"):
        passed(2, None, pair)
        twins(1, None, pair)
    with jax.named_scope("down0"):
        lower(1 - y, 0, early)
    for d in order[:2]:
        across_y(d, early).start()
    with jax.named_scope("hide1"):
        hide(y, 1)
    with jax.named_scope("down1"):
        lower(y, 1, early)
    with jax.named_scope("wh"):
        passed(2, edge_z, inner_z)
        twins(1, edge_z, inner_z)
    with jax.named_scope("down2"):
        lower(1 - y, 0, late)
    for d in order[:2]:
        across_y(d, late).start()
    for d in order[2:]:
        for h in (early, late):
            across_y(d, h).start()
    with jax.named_scope("down3"):
        lower(y, 1, late)
    for i, h in ((0, early), (1, early), (0, late), (1, late), (2, early), (2, late)):
        with jax.named_scope("rs%d%d" % (i, h is late)):
            step(i, h)
    with jax.named_scope("rsend0"):
        gather_in(z, early, z > 0, z < deep - 1)
    with jax.named_scope("rsend1"):
        gather_in(z, late, z > 0, z < deep - 1)
    with jax.named_scope("fin"):
        finished = layer_norm(
            ALPHA * rows[y, z].astype(jnp.float32) + 0.5 * acc[...], gain[...], shift[...]
        )
        out[core] = finished.astype(jnp.bfloat16)
    last = remote(out.at[core], out.at[core], f_sem.at[0, 0], f_sem.at[1, 0], twin)
    last.start()

    with jax.named_scope("drain"):

        @pl.when(z < deep - 1)
        def _():
            to_next().wait_send()

        for dy, dz in sides:
            for mat in range(3):
                bring(mat, dy, dz, lambda copy: copy.wait_send())
                if (dy, dz) != (0, 0):
                    relay(mat, dy, dz, lambda copy: copy.wait_send())
            for j in range(2):
                for k in range(2):
                    share(j, k, dy, dz).wait_send()
        for dp in range(1, plane):
            for copy in (*to_plane(dp), to_fellow(dp)):
                copy.wait_send()
        for zz in range(deep):

            for h in halves:

                @pl.when(jnp.logical_and(zz <= z, z < deep - 1))
                def _():
                    climb(zz, h).wait_send()

                @pl.when(jnp.logical_and(zz >= z, z > 0))
                def _():
                    sink(zz, h).wait_send()

                cross_y(zz, h).wait_send()
                across_y(zz, h).wait_send()
        for h in halves:
            for i in range(deep - 1):
                hop(i, h, True).wait_send()
        last.wait()


def layer(
    resid,
    queries,
    keys,
    values,
    decay_pre,
    out_gate,
    head_gain,
    out_proj,
    mix_gain,
    mix_shift,
    gate_in,
    up_in,
    down_out,
    gain,
    shift,
):
    count = lax.axis_size("sp")
    tok_rows, inner = resid.shape
    own = tok_rows // 2
    deep = count // 4
    groups = count // 2
    wide = -(-(gate_in.shape[1] // LANES) // groups)
    span = wide * LANES
    heads = queries.shape[1] // HK
    steps = tok_rows // SPAN
    dma = pltpu.SemaphoreType.DMA
    half, full = jnp.bfloat16, jnp.float32
    block = lambda *lead: pltpu.VMEM((*lead, own, inner), half)
    near, far = pl.BlockSpec(memory_space=pltpu.VMEM), pl.BlockSpec(memory_space=pl.ANY)
    out = pl.pallas_call(
        functools.partial(layer_kernel, deep, wide),
        out_shape=pltpu.VMEM((2, own, inner), half),
        in_specs=[far] * 5 + [near] + [far] * 2 + [near] * 2 + [far] * 3 + [near] * 2,
        out_specs=near,
        scratch_shapes=[
            pltpu.VMEM(queries.shape, half),
            pltpu.VMEM(keys.shape, half),
            pltpu.VMEM(values.shape, half),
            pltpu.VMEM(decay_pre.shape, full),
            pltpu.VMEM(out_gate.shape, half),
            block(2),
            pltpu.VMEM((2, inner, 2 * span), half),
            pltpu.VMEM((2 * span, inner), half),
            pltpu.VMEM(out_proj.shape, half),
            pltpu.VMEM((steps, heads, HK, HV), full),
            pltpu.VMEM((steps, heads, HK, HK), full),
            pltpu.VMEM((heads, HK, HV), half),
            pltpu.VMEM((heads, 8, HK), full),
            pltpu.VMEM((4, HK, HV), half),
            pltpu.VMEM((4, 8, HK), full),
            pltpu.VMEM((4, HK, HV), full),
            pltpu.VMEM((HK, HV), full),
            pltpu.VMEM((HK, HV), half),
            pltpu.VMEM((HK, HV), half),
            pltpu.VMEM((4, HK, HV), half),
            pltpu.VMEM((4, HK, HV), half),
            pltpu.VMEM((tok_rows, out_proj.shape[0]), half),
            block(2),
            block(),
            block(2, deep),
            pltpu.VMEM((2, deep * own, 2 * span), half),
            block(2, deep),
            block(deep),
            block(deep),
            block(deep),
            block(deep - 1),
            pltpu.VMEM((own, inner), full),
            dma((4,)),
            dma((3, groups)),
            dma((3, groups)),
            dma((3, groups)),
            dma((3, groups)),
            dma((2, 2, groups)),
            dma((2, 2, groups)),
            dma((4, 2)),
            dma((4, 2)),
            dma((2,)),
            dma((4,)),
            dma((4,)),
            dma((2,)),
            *[dma((deep, 2))] * 10,
            dma((2, 2)),
            pltpu.SemaphoreType.REGULAR,
            dma((6,)),
        ],
        compiler_params=pltpu.CompilerParams(
            collective_id=2, has_side_effects=True, vmem_limit_bytes=60 * 1024 * 1024
        ),
    )(
        queries,
        keys,
        values,
        decay_pre,
        out_gate,
        head_gain[None],
        out_proj,
        resid.reshape(2, own, inner),
        mix_gain[None],
        mix_shift[None],
        gate_in,
        up_in,
        down_out,
        gain[None],
        shift[None],
    )
    return out.reshape(tok_rows, inner)


def body(
    resid,
    queries,
    keys,
    values,
    decay_pre,
    out_gate,
    head_gain,
    out_proj,
    mix_gain,
    mix_shift,
    gate_in,
    up_in,
    down_out,
    out_gain,
    out_shift,
):
    tp_count = lax.axis_size("tp")
    tok_rows = queries.shape[0]
    own_count = tok_rows // tp_count
    sp_count = lax.axis_size("sp")
    units = gate_in.shape[1]
    heads = queries.shape[1] // HK
    groups = sp_count // 2
    unit_blocks = units // LANES
    by_units = (
        tp_count == 2
        and sp_count == 16
        and heads == 4
        and units % LANES == 0
        and unit_blocks % groups == groups - 2
        and gate_in.shape[0] % LANES == 0
        and down_out.shape[1] % LANES == 0
        and gate_in.shape[0] * sp_count == resid.shape[1]
        and own_count % 16 == 0
        and tok_rows % SPAN == 0
    )
    if by_units:
        return layer(
            resid,
            queries,
            keys,
            values,
            decay_pre,
            out_gate,
            head_gain,
            out_proj,
            mix_gain,
            mix_shift,
            gate_in,
            up_in,
            down_out,
            out_gain,
            out_shift,
        )
    local = local_tokens(queries, keys, values, decay_pre)
    gated = mix_tokens(*local, out_gate, head_gain)
    mixed = lax.psum_scatter(
        jnp.dot(gated, out_proj, preferred_element_type=jnp.float32).astype(jnp.bfloat16),
        "tp",
        scatter_dimension=0,
        tiled=True,
    ).astype(jnp.float32)
    own_resid = lax.dynamic_slice_in_dim(resid, lax.axis_index("tp") * own_count, own_count, 0)
    mid = layer_norm(ALPHA * own_resid.astype(jnp.float32) + mixed, mix_gain, mix_shift).astype(
        jnp.bfloat16
    )
    whole_rows = lax.all_gather(mid, "tp", axis=0, tiled=True)
    hidden = hidden_by_rows(whole_rows, gate_in, up_in)
    ffn = lax.psum_scatter(
        down_by_columns(hidden, down_out).astype(jnp.bfloat16),
        "tp",
        scatter_dimension=0,
        tiled=True,
    ).astype(jnp.float32)
    finished = layer_norm(ALPHA * mid.astype(jnp.float32) + 0.5 * ffn, out_gain, out_shift).astype(
        jnp.bfloat16
    )
    return lax.all_gather(finished, "tp", axis=0, tiled=True)


def solution(mesh):
    return jax.shard_map(
        body,
        mesh=mesh,
        in_specs=(
            P("sp", None),
            P("sp", "tp"),
            P("sp", "tp"),
            P("sp", "tp"),
            P("sp", "tp"),
            P("sp", "tp"),
            P(),
            P("tp", None),
            P(),
            P(),
            P("sp", "tp"),
            P("sp", "tp"),
            P("tp", "sp"),
            P(),
            P(),
        ),
        out_specs=P("sp", None),
        check_vma=False,
    )
```

```python
import functools

import jax
import jax.numpy as jnp
from jax import lax
from jax.experimental import pallas as pl
from jax.experimental.pallas import tpu as pltpu
from jax.sharding import PartitionSpec as P

HK = 128
HV = 256
SPAN = 64
LANES = 128


ALPHA = 2.0**0.25
LN_EPS = 1e-05
RMS_EPS = 1e-06
TAU = 16.0
MESH = pl.DeviceIdType.MESH


def entering(array, axis, combine, identity):
    count, place = (lax.axis_size(axis), lax.axis_index(axis))
    everything = jax.tree.map(
        lambda part, kind: lax.all_gather(part.astype(kind), axis),
        array,
        (jnp.bfloat16, jnp.bfloat16),
    )
    start = jax.tree.map(
        lambda part, zero: jnp.broadcast_to(jnp.asarray(zero, part.dtype), part.shape),
        array,
        identity,
    )

    def lap(k, before):
        reached = k < place
        new = combine(
            before, jax.tree.map(lambda part, own: part[k].astype(own.dtype), everything, array)
        )
        return jax.tree.map(lambda a, b: jnp.where(reached, a, b), new, before)

    return lax.fori_loop(0, count, lap, start)


def layer_norm(inputs, gain, shift):
    center = inputs - jnp.mean(inputs, axis=-1, keepdims=True)
    spread = jnp.mean(center * center, axis=-1, keepdims=True)
    return center * lax.rsqrt(spread + LN_EPS) * gain + shift


def combine_states(earlier, later):
    return (earlier[0] * later[0], later[0][..., None] * earlier[1] + later[1])


def greet(places):
    barrier = pltpu.get_barrier_semaphore()
    for place in places:
        pl.semaphore_signal(barrier, inc=1, device_id=place, device_id_type=MESH)
    pl.semaphore_wait(barrier, len(places))


def remote(src, dst, send, recv, place):
    return pltpu.make_async_remote_copy(
        src_ref=src, dst_ref=dst, send_sem=send, recv_sem=recv, device_id=place, device_id_type=MESH
    )


def local_tokens(queries, keys, values, decay_pre):
    tok_rows = queries.shape[0]
    local_heads = queries.shape[1] // HK
    blocks = tok_rows // SPAN
    logdecay = jax.nn.log_sigmoid(decay_pre) / TAU
    scaled_q = queries.astype(jnp.float32).reshape(blocks, SPAN, local_heads, HK) * HK ** (-0.5)
    key_block = keys.astype(jnp.float32).reshape(blocks, SPAN, local_heads, HK)
    value_block = values.astype(jnp.float32).reshape(blocks, SPAN, local_heads, HV)
    cumul = jnp.cumsum(logdecay.reshape(blocks, SPAN, local_heads, HK), axis=1)
    last = cumul[:, -1]
    key_decayed = key_block * jnp.exp(last[:, None] - cumul)
    updates = jnp.einsum(
        "nchk,nchv->nhkv", key_decayed, value_block, precision=lax.Precision.HIGHEST
    )

    def advance(running_state, inputs):
        decay_end, state_increment, current_query = inputs
        running_state = jnp.exp(decay_end)[..., None] * running_state + state_increment
        return (
            running_state,
            jnp.einsum(
                "qpy,pyr->qpr", current_query, running_state, precision=lax.Precision.HIGHEST
            ),
        )

    own_state, local_read = lax.scan(
        advance, jnp.zeros((local_heads, HK, HV), jnp.float32), (last, updates, scaled_q)
    )
    block_ends = jnp.cumsum(last, axis=0)
    own_decay = jnp.exp(block_ends[-1])
    carry_q = scaled_q * jnp.exp(block_ends)[:, None]
    return local_read, carry_q, own_decay, own_state


def mix_tokens(local_read, carry_q, own_decay, own_state, out_gate, head_gain):
    blocks, span, local_heads, _ = carry_q.shape
    tok_rows = blocks * span
    identity = (jnp.ones_like(own_decay), jnp.zeros_like(own_state))
    _, incoming = entering((own_decay, own_state), "sp", combine_states, identity)
    carried = jnp.einsum(
        "xepj,pjw->xepw", carry_q, incoming, precision=lax.Precision.HIGHEST
    )
    state_readout = (local_read + carried).reshape(tok_rows, local_heads, HV)
    normed = (
        state_readout
        * lax.rsqrt(jnp.mean(state_readout * state_readout, axis=-1, keepdims=True) + RMS_EPS)
        * head_gain
    )
    return (
        normed.reshape(tok_rows, local_heads * HV) * jax.nn.silu(out_gate.astype(jnp.float32))
    ).astype(jnp.bfloat16)


def hidden_by_rows(whole_rows, gate_in, up_in):
    gate = jnp.dot(
        whole_rows,
        lax.all_gather(gate_in, "sp", axis=0, tiled=True),
        preferred_element_type=jnp.float32,
    )
    upward = jnp.dot(
        whole_rows,
        lax.all_gather(up_in, "sp", axis=0, tiled=True),
        preferred_element_type=jnp.float32,
    )
    return (jax.nn.silu(gate) * upward).astype(jnp.bfloat16)


def down_by_columns(hidden, down_out):
    return jnp.dot(
        hidden,
        lax.all_gather(down_out, "sp", axis=1, tiled=True),
        preferred_element_type=jnp.float32,
    )


def layer_kernel(
    deep,
    wide,
    queries_far,
    keys_far,
    values_far,
    decay_pre_far,
    out_gate_far,
    head_gain,
    out_proj,
    resid_far,
    mix_gain,
    mix_shift,
    gate_in,
    up_in,
    down_out,
    gain,
    shift,
    out,
    queries,
    keys,
    values,
    decay_pre,
    out_gate,
    resid,
    w1,
    w2,
    proj,
    updates,
    ends,
    s_out,
    d_out,
    s_in,
    d_in,
    before,
    total,
    t_out,
    t_in,
    s_start,
    start,
    gated,
    mixed,
    mixed_in,
    rows,
    hidden,
    part,
    y_in,
    u_in,
    v_in,
    z_out,
    acc,
    own_sem,
    b_send,
    b_recv,
    f_send,
    f_recv,
    t_send,
    t_recv,
    p1_send,
    p1_recv,
    p2_sem,
    p3_send,
    p3_recv,
    m_sem,
    au_send,
    av_send,
    ay_send,
    az_recv,
    ay_recv,
    ry_send,
    ry_recv,
    rz_send,
    ru_recv,
    rv_recv,
    f_sem,
    go_sem,
    near_sem,
):
    me, core = lax.axis_index("sp"), lax.axis_index("tp")
    x, y, z = me % 2, (me // 2) % 2, me // 4
    group = me // 2
    groups = 2 * deep
    plane = 4
    place = me % plane
    own, inner = rows.shape[2], rows.shape[3]
    depth = gate_in.shape[0]
    lanes = down_out.shape[1]
    span = wide * LANES
    half = lambda c: pl.ds(pl.multiple_of(c * span, span), span)
    twin = (me, 1 - core)
    x_place = (me + 1 - 2 * x, core)
    y_place = (me + 2 - 4 * y, core)
    above, below = (me + plane, core), (me - plane, core)
    sides = [(dy, dz) for dz in range(deep) for dy in range(2)]
    bottom = z < deep // 2
    edge = jnp.logical_or(z == 0, z == deep - 1)
    pair = z + 1 - 2 * (z % 2)
    inner_z = jnp.where(bottom, deep // 2, deep // 2 - 1)
    edge_z = jnp.where(bottom, deep - 1, 0)

    def at(xx, yy, zz):
        return (plane * zz + 2 * yy + xx, core)

    def target(dy, dz):
        return (y + dy) % 2, (z + dz) % deep

    def origin(dy, dz):
        return (y + dy) % 2, (z + deep - dz) % deep

    def fellow(dp):
        return (x + dp % 2) % 2, (y + dp // 2) % 2

    def short(c, g):
        return jnp.logical_or(g == c, g == groups - 2 + c)

    def first_block(c, g):
        return wide * g - (g > c).astype(jnp.int32) - (g > groups - 2 + c).astype(jnp.int32)

    def sized(flag, run):
        @pl.when(flag)
        def _():
            run(wide - 1)

        @pl.when(jnp.logical_not(flag))
        def _():
            run(wide)

    def taken(mat, g, blocks):
        begin = pl.ds(pl.multiple_of(first_block(core, g) * LANES, LANES), blocks * LANES)
        return (gate_in.at[:, begin], up_in.at[:, begin], down_out.at[begin])[mat]

    def landing(mat, c, s, blocks):
        if mat < 2:
            rows_of = pl.ds(pl.multiple_of(s * depth, depth), depth)
            return w1.at[c, rows_of, pl.ds(mat * span, blocks * LANES)]
        columns = pl.ds(pl.multiple_of(s * lanes, lanes), lanes)
        return w2.at[pl.ds(pl.multiple_of(c * span, span), blocks * LANES), columns]

    def slab(j, c, s):
        if j == 0:
            return w1.at[c, pl.ds(pl.multiple_of(s * depth, depth), depth)]
        return landing(2, c, s, wide)

    def home(dy, dz):
        return isinstance(dz, int) and dy == 0 and dz == 0

    def bring(mat, dy, dz, run):
        yy, zz = target(dy, dz)
        goal = x_place if home(dy, dz) else at(x, yy, zz)
        g = 2 * zz + yy
        r = 2 * dz + dy

        def copy(blocks):
            run(
                remote(
                    taken(mat, g, blocks),
                    landing(mat, core, me, blocks),
                    b_send.at[mat, r],
                    b_recv.at[mat, r],
                    goal,
                )
            )

        sized(short(core, g), copy)

    def send(mat, dy, dz):
        bring(mat, dy, dz, lambda copy: copy.start())

    def send_near(mat):
        send(mat, 0, 0)
        send(mat, 1, 0)

    def send_to(mat, dy, zz):
        send(mat, dy, (zz + deep - z) % deep)

    def source(dy, dz, k):
        yy, zz = origin(dy, dz)
        return plane * zz + 2 * yy + (x + k) % 2

    def relay(mat, dy, dz, run):
        r = 2 * dz + dy

        def copy(blocks):
            block = landing(mat, core, source(dy, dz, 0), blocks)
            run(remote(block, block, f_send.at[mat, r], f_recv.at[mat, r], x_place))

        sized(short(core, group), copy)

    def share(j, k, dy, dz):
        block = slab(j, core, source(dy, dz, k))
        r = 2 * dz + dy
        return remote(block, block, t_send.at[j, k, r], t_recv.at[j, k, r], twin)

    def came(ref, sem):
        remote(ref, ref, f_sem.at[0, 0], sem, twin).wait_recv()

    def shared(mat, k, dy, dz):
        if mat:
            share(mat - 1, k, dy, dz).start()

    def pass_on(mat, dy, dz):
        k = 1 if home(dy, dz) else 0
        sized(
            short(core, group),
            lambda blocks: came(
                landing(mat, core, source(dy, dz, k), blocks), b_recv.at[mat, 2 * dz + dy]
            ),
        )
        if not k:
            relay(mat, dy, dz, lambda copy: copy.start())
        shared(mat, k, dy, dz)

    def pass_on_near(mat):
        pass_on(mat, 0, 0)
        pass_on(mat, 1, 0)

    def pass_on_from(mat, dy, zz):
        pass_on(mat, dy, (z + deep - zz) % deep)

    def passed(mat, *levels):
        def one(dy, dz):
            sized(
                short(core, group),
                lambda blocks: came(
                    landing(mat, core, source(dy, dz, 1), blocks), f_recv.at[mat, 2 * dz + dy]
                ),
            )
            shared(mat, 1, dy, dz)

        for zz in levels:
            if zz is None:
                one(1, 0)
            else:
                for dy in range(2):
                    one(dy, (z + deep - zz) % deep)

    def local(mat, run):
        def copy(blocks):
            run(
                pltpu.make_async_copy(
                    taken(mat, group, blocks), landing(mat, core, me, blocks), own_sem.at[mat]
                )
            )

        sized(short(core, group), copy)

    keep_proj = pltpu.make_async_copy(out_proj, proj, own_sem.at[3])

    keep_near = [
        pltpu.make_async_copy(ref, copy, near_sem.at[i])
        for i, (ref, copy) in enumerate(
            (
                (decay_pre_far, decay_pre),
                (keys_far, keys),
                (values_far, values),
                (queries_far, queries),
                (out_gate_far, out_gate),
                (resid_far, resid),
            )
        )
    ]
    for copy in keep_near:
        copy.start()

    with jax.named_scope("greet"):
        partners = [at(x, *target(dy, dz)) for dy, dz in sides[1:]]
        partners += [x_place, at(*fellow(3), z), twin]
        greet(partners)
    for zz in (inner_z, edge_z, pair):
        send_to(0, 0, zz)
    for mat in range(3):
        local(mat, lambda copy: copy.start())
    keep_proj.start()

    with jax.named_scope("local"):
        for copy in keep_near[:3]:
            copy.wait()
        tokens = queries.shape[0]
        heads = queries.shape[1] // HK
        blocks = tokens // SPAN
        raw = decay_pre[...]
        logdecay = (jnp.minimum(raw, 0.0) - jnp.log1p(jnp.exp(-jnp.abs(raw)))) / TAU
        row = lax.broadcasted_iota(jnp.int32, (tokens, tokens), 0)
        col = lax.broadcasted_iota(jnp.int32, (tokens, tokens), 1)
        tri = jnp.logical_and(row // SPAN == col // SPAN, col <= row).astype(jnp.float32)
        cumul = jnp.dot(
            tri, logdecay, precision=lax.Precision.HIGHEST, preferred_element_type=jnp.float32
        )
        lasts = [cumul[(n + 1) * SPAN - 1 : (n + 1) * SPAN] for n in range(blocks)]
        across = (((0,), (0,)), ((), ()))

        def column(line):
            return jnp.broadcast_to(line, (HK, HK)).T

        def spread(square):
            return jnp.concatenate([square] * (HV // HK), axis=1)

        for n in range(blocks):
            steps = slice(n * SPAN, (n + 1) * SPAN)
            faded = keys[steps].astype(jnp.float32) * jnp.exp(lasts[n] - cumul[steps])
            high = faded.astype(jnp.bfloat16)
            low = (faded - high.astype(jnp.float32)).astype(jnp.bfloat16)
            for h in range(heads):
                key = slice(h * HK, (h + 1) * HK)
                value = values[steps, h * HV : (h + 1) * HV]
                updates[n, h] = lax.dot_general(
                    high[:, key], value, across, preferred_element_type=jnp.float32
                ) + lax.dot_general(
                    low[:, key], value, across, preferred_element_type=jnp.float32
                )
                ends[n, h] = column(jnp.exp(lasts[n][:, key]))
        whole = jnp.exp(sum(lasts))
        for h in range(heads):
            state = updates[0, h]
            for n in range(1, blocks):
                state = spread(ends[n, h]) * state + updates[n, h]
            s_out[h] = state.astype(jnp.bfloat16)
            d_out[h] = jnp.broadcast_to(whole[:, h * HK : (h + 1) * HK], d_out.shape[1:])

    def to_plane(dp):
        xx, yy = fellow(dp)
        goal, slot = at(xx, yy, z), 2 * yy + xx
        return (
            remote(s_out.at[slot], s_in.at[place], p1_send.at[dp, 0], p1_recv.at[dp, 0], goal),
            remote(d_out.at[slot], d_in.at[place], p1_send.at[dp, 1], p1_recv.at[dp, 1], goal),
        )

    for dp in range(1, plane):
        for copy in to_plane(dp):
            copy.start()
    s_in[place] = s_out[place]
    d_in[place] = d_out[place]
    send_near(0)

    @pl.when(short(core, group))
    def _():
        last_block = (wide - 1) * LANES
        blank = jnp.zeros((w1.shape[1], LANES), jnp.bfloat16)
        w1[core, :, last_block:span] = blank
        w1[core, :, span + last_block :] = blank
        tail = pl.ds(pl.multiple_of(core * span + last_block, LANES), LANES)
        w2[tail] = jnp.zeros((LANES, inner), jnp.bfloat16)

    with jax.named_scope("p1"):
        for dp in range(1, plane):
            for copy in to_plane(dp):
                copy.wait_recv()
    running = jnp.zeros((HK, HV), jnp.float32)
    line = jnp.ones((1, HK), jnp.float32)
    reach = []
    for i in range(plane):
        before[i] = running
        reach.append(line)
        own_decay = d_in[i][:1]
        running = spread(column(own_decay)) * running + s_in[i].astype(jnp.float32)
        line = line * own_decay
    total[...] = jnp.zeros(total.shape, jnp.float32)

    def to_next():
        return remote(t_out, t_in, p2_sem.at[0], p2_sem.at[1], above)

    def push_on():
        t_out[...] = (spread(column(line)) * total[...] + running).astype(jnp.bfloat16)
        to_next().start()

    @pl.when(z == 0)
    def _():
        push_on()

    @pl.when(jnp.logical_not(bottom))
    def _():
        for mat, dy, zz in ((1, 0, inner_z), (1, 0, edge_z), (0, 1, inner_z)):
            send_to(mat, dy, zz)

    def gates():
        pass_on_near(0)
        for zz in (pair, edge_z, inner_z):
            pass_on_from(0, 0, zz)

    with jax.named_scope("gates1"):

        @pl.when(jnp.logical_not(bottom))
        def _():
            gates()

    with jax.named_scope("p2"):

        @pl.when(z > 0)
        def _():
            came(t_in, p2_sem.at[1])
            total[...] = t_in[...].astype(jnp.float32)

    @pl.when(jnp.logical_and(z > 0, z < deep - 1))
    def _():
        push_on()

    for i in range(plane):
        s_start[i] = (before[i] + spread(column(reach[i])) * total[...]).astype(jnp.bfloat16)

    def to_fellow(dp):
        xx, yy = fellow(dp)
        slot = 2 * yy + xx
        return remote(
            s_start.at[slot], start.at[place], p3_send.at[dp], p3_recv.at[dp], at(xx, yy, z)
        )

    for dp in range(1, plane):
        to_fellow(dp).start()
    start[place] = s_start[place]
    send_to(1, 0, pair)
    send_to(2, 0, pair)
    send_to(0, 1, pair)

    @pl.when(bottom)
    def _():
        for zz in (inner_z, edge_z):
            send_to(1, 0, zz)
            send_to(0, 1, zz)

    @pl.when(jnp.logical_not(bottom))
    def _():
        send_to(0, 1, edge_z)

    send_near(1)
    send_near(2)
    with jax.named_scope("gates2"):

        @pl.when(bottom)
        def _():
            gates()

    with jax.named_scope("p3"):
        for dp in range(1, plane):
            to_fellow(dp).wait_recv()

    with jax.named_scope("mix"):
        for copy in keep_near[3:]:
            copy.wait()
        for h in range(heads):
            thick = slice(h * HV, (h + 1) * HV)
            state = start[h].astype(jnp.float32)
            reads = []
            for n in range(blocks):
                state = spread(ends[n, h]) * state + updates[n, h]
                high = state.astype(jnp.bfloat16)
                low = (state - high.astype(jnp.float32)).astype(jnp.bfloat16)
                query = queries[n * SPAN : (n + 1) * SPAN, h * HK : (h + 1) * HK]
                reads.append(
                    jnp.dot(query, high, preferred_element_type=jnp.float32)
                    + jnp.dot(query, low, preferred_element_type=jnp.float32)
                )
            read = jnp.concatenate(reads, axis=0) * HK ** (-0.5)
            size = jnp.mean(read * read, axis=-1, keepdims=True)
            pre = out_gate[:, thick].astype(jnp.float32)
            normed = read * lax.rsqrt(size + RMS_EPS) * head_gain[...]
            gated[:, thick] = (normed * (pre * jax.nn.sigmoid(pre))).astype(jnp.bfloat16)
    keep_proj.wait()
    with jax.named_scope("proj"):
        summed_heads = jnp.dot(gated[...], proj[...], preferred_element_type=jnp.float32)
        mixed[...] = summed_heads.astype(jnp.bfloat16).reshape(2, own, inner)
    swap = remote(mixed.at[1 - core], mixed_in, m_sem.at[0], m_sem.at[1], twin)
    swap.start()
    with jax.named_scope("swap"):
        swap.wait()
    with jax.named_scope("ln"):
        added = mixed[core].astype(jnp.float32) + mixed_in[...].astype(jnp.float32)
        middle = ALPHA * resid[core].astype(jnp.float32) + added
        rows[y, z] = layer_norm(middle, mix_gain[...], mix_shift[...]).astype(jnp.bfloat16)

    halves = range(2)
    chunk = own // 2
    bit = [pl.ds(h * chunk, chunk) for h in halves]

    def climb(zz, h):
        block = rows.at[y, zz, bit[h]]
        return remote(block, block, au_send.at[zz, h], az_recv.at[zz, h], above)

    def sink(zz, h):
        block = rows.at[y, zz, bit[h]]
        return remote(block, block, av_send.at[zz, h], az_recv.at[zz, h], below)

    def cross_y(zz, h):
        block = rows.at[y, zz, bit[h]]
        return remote(block, block, ay_send.at[zz, h], ay_recv.at[zz, h], y_place)

    for h in halves:

        @pl.when(z < deep - 1)
        def _():
            climb(z, h).start()

        @pl.when(z > 0)
        def _():
            sink(z, h).start()

        cross_y(z, h).start()

    ahead = jnp.logical_not(jnp.logical_or(bottom, edge))

    @pl.when(ahead)
    def _():
        for zz in (inner_z, edge_z):
            send_to(1, 1, zz)

    def landed(far):
        for h in halves:

            @pl.when(z >= far)
            def _():
                came(rows.at[y, z - far, bit[h]], az_recv.at[z - far, h])

                @pl.when(z < deep - 1)
                def _():
                    climb(z - far, h).start()

                cross_y(z - far, h).start()

            @pl.when(z < deep - far)
            def _():
                came(rows.at[y, z + far, bit[h]], az_recv.at[z + far, h])

                @pl.when(z > 0)
                def _():
                    sink(z + far, h).start()

                cross_y(z + far, h).start()

    with jax.named_scope("wa"):
        for mat in range(3):
            local(mat, lambda copy: copy.wait())
        share(0, 0, 0, 0).start()
        share(1, 0, 0, 0).start()
        pass_on_near(1)
        for zz in (pair, edge_z, inner_z):
            pass_on_from(1, 0, zz)
        pass_on_from(0, 1, pair)
        pass_on_from(2, 0, pair)
    with jax.named_scope("ag1"):
        landed(1)

    send_to(1, 1, pair)
    send_to(2, 1, pair)

    def second_wave():
        @pl.when(jnp.logical_not(ahead))
        def _():
            for zz in (inner_z, edge_z):
                send_to(1, 1, zz)

        for dy in range(2):
            for zz in (inner_z, edge_z):
                send_to(2, dy, zz)

    @pl.when(jnp.logical_not(edge))
    def _():
        second_wave()

    with jax.named_scope("wb"):
        for zz in (edge_z, inner_z):
            pass_on_from(0, 1, zz)
        pass_on_near(2)
    with jax.named_scope("ag2"):
        landed(2)

    @pl.when(jnp.logical_not(edge))
    def _():
        pl.semaphore_signal(
            go_sem, inc=1, device_id=at(x, y, edge_z), device_id_type=MESH
        )

    with jax.named_scope("wc"):
        pass_on_from(1, 1, pair)
        pass_on_from(2, 1, pair)

    with jax.named_scope("go"):

        @pl.when(edge)
        def _():
            pl.semaphore_wait(go_sem, 1)
            second_wave()

    with jax.named_scope("ag3"):
        for far in range(3, deep):
            landed(far)
    with jax.named_scope("wd0"):
        passed(0, None, pair, edge_z, inner_z)
        passed(1, None, pair)
    with jax.named_scope("wd"):
        pass_on_from(1, 1, inner_z)
        pass_on_from(1, 1, edge_z)
        passed(2, None, pair)
        pass_on_from(2, 0, edge_z)
        pass_on_from(2, 0, inner_z)
    def last_blocks():
        pass_on_from(2, 1, edge_z)
        pass_on_from(2, 1, inner_z)

    with jax.named_scope("we"):

        @pl.when(jnp.logical_not(bottom))
        def _():
            last_blocks()

    with jax.named_scope("wf"):
        passed(1, edge_z, inner_z)
    with jax.named_scope("agy"):
        for zz in range(deep):
            for h in halves:
                came(rows.at[1 - y, zz, bit[h]], ay_recv.at[zz, h])
    def twins(j, *levels):
        for zz in levels:
            dz = 0 if zz is None else (z + deep - zz) % deep
            for k in range(2):
                for dy in range(2):
                    came(slab(j, 1 - core, source(dy, dz, k)), t_recv.at[j, k, 2 * dz + dy])

    with jax.named_scope("wt"):
        twins(0, None, pair, edge_z, inner_z)

    def hide(side, slot):
        left = rows[side].reshape(deep * own, inner)
        for c in range(2):
            both = jnp.dot(left, w1[c], preferred_element_type=jnp.float32)
            gate, up = both[:, :span], both[:, span:]
            hidden[slot, :, c * span : (c + 1) * span] = (
                gate * jax.nn.sigmoid(gate) * up
            ).astype(jnp.bfloat16)

    wing = inner // 2
    early = jnp.where(bottom, 0, 1)
    late = 1 - early
    columns = lambda h: pl.ds(pl.multiple_of(h * wing, wing), wing)

    def lower(side, slot, h):
        down = jnp.dot(hidden[slot], w2[:, columns(h)], preferred_element_type=jnp.float32)
        part[side, :, :, columns(h)] = down.astype(jnp.bfloat16).reshape(deep, own, wing)

    order = [
        jnp.where(bottom, deep - 1, 0),
        jnp.where(bottom, deep - 2, 1),
        jnp.where(bottom, 1 - z, 2 * deep - 3 - z),
        z,
    ]

    slim = wing // 2
    columns_of = lambda q: pl.ds(pl.multiple_of(q * slim, slim), slim)
    quarters = lambda h: (2 * h, 2 * h + 1)

    def across_y(d, h):
        return remote(
            part.at[1 - y, d, :, columns_of(h)],
            y_in.at[d, :, columns_of(h)],
            ry_send.at[d, h],
            ry_recv.at[d, h],
            y_place,
        )

    def hop(i, h, up):
        into, sem = (u_in, ru_recv) if up else (v_in, rv_recv)
        return remote(
            z_out.at[i, :, columns_of(h)],
            into.at[order[i], :, columns_of(h)],
            rz_send.at[i, h],
            sem.at[order[i], h],
            above if up else below,
        )

    def gather_in(d, h, from_below, from_above):
        taken = columns_of(h)
        came(y_in.at[d, :, taken], ry_recv.at[d, h])
        acc[:, taken] = part[y, d, :, taken].astype(jnp.float32) + y_in[d, :, taken].astype(
            jnp.float32
        )

        @pl.when(from_below)
        def _():
            came(u_in.at[d, :, taken], ru_recv.at[d, h])
            acc[:, taken] += u_in[d, :, taken].astype(jnp.float32)

        @pl.when(from_above)
        def _():
            came(v_in.at[d, :, taken], rv_recv.at[d, h])
            acc[:, taken] += v_in[d, :, taken].astype(jnp.float32)

    def step(i, h):
        d = order[i]
        up = d > z
        gather_in(
            d,
            h,
            jnp.logical_and(up, z > 0),
            jnp.logical_and(jnp.logical_not(up), z < deep - 1),
        )
        z_out[i, :, columns_of(h)] = acc[:, columns_of(h)].astype(jnp.bfloat16)

        @pl.when(up)
        def _():
            hop(i, h, True).start()

        @pl.when(jnp.logical_not(up))
        def _():
            hop(i, h, False).start()

    with jax.named_scope("hide0"):
        hide(1 - y, 0)
    with jax.named_scope("wx"):

        @pl.when(bottom)
        def _():
            last_blocks()

    with jax.named_scope("wg"):
        twins(1, None, pair)
    with jax.named_scope("down0"):
        lower(1 - y, 0, early)
    for d in order[:2]:
        for q in quarters(early):
            across_y(d, q).start()
    with jax.named_scope("hide1"):
        hide(y, 1)
    with jax.named_scope("down1"):
        lower(y, 1, early)
    with jax.named_scope("wh"):
        passed(2, edge_z, inner_z)
        twins(1, edge_z, inner_z)
    with jax.named_scope("down2"):
        lower(1 - y, 0, late)
    for d in order[:2]:
        for q in quarters(late):
            across_y(d, q).start()
    for d in order[2:]:
        for h in (early, late):
            for q in quarters(h):
                across_y(d, q).start()
    with jax.named_scope("down3"):
        lower(y, 1, late)
    for i, h in ((0, early), (1, early), (0, late), (1, late), (2, early), (2, late)):
        with jax.named_scope("rs%d%d" % (i, h is late)):
            for q in quarters(h):
                step(i, q)
    with jax.named_scope("rsend0"):
        for q in quarters(early):
            gather_in(z, q, z > 0, z < deep - 1)
    with jax.named_scope("rsend1"):
        for q in quarters(late):
            gather_in(z, q, z > 0, z < deep - 1)
    with jax.named_scope("fin"):
        finished = layer_norm(
            ALPHA * rows[y, z].astype(jnp.float32) + 0.5 * acc[...], gain[...], shift[...]
        )
        out[core] = finished.astype(jnp.bfloat16)
    last = remote(out.at[core], out.at[core], f_sem.at[0, 0], f_sem.at[1, 0], twin)
    last.start()

    with jax.named_scope("drain"):

        @pl.when(z < deep - 1)
        def _():
            to_next().wait_send()

        for dy, dz in sides:
            for mat in range(3):
                bring(mat, dy, dz, lambda copy: copy.wait_send())
                if (dy, dz) != (0, 0):
                    relay(mat, dy, dz, lambda copy: copy.wait_send())
            for j in range(2):
                for k in range(2):
                    share(j, k, dy, dz).wait_send()
        for dp in range(1, plane):
            for copy in (*to_plane(dp), to_fellow(dp)):
                copy.wait_send()
        for zz in range(deep):

            for h in halves:

                @pl.when(jnp.logical_and(zz <= z, z < deep - 1))
                def _():
                    climb(zz, h).wait_send()

                @pl.when(jnp.logical_and(zz >= z, z > 0))
                def _():
                    sink(zz, h).wait_send()

                cross_y(zz, h).wait_send()
        for q in range(4):
            for i in range(deep):
                across_y(i, q).wait_send()
            for i in range(deep - 1):
                hop(i, q, True).wait_send()
        last.wait()


def layer(
    resid,
    queries,
    keys,
    values,
    decay_pre,
    out_gate,
    head_gain,
    out_proj,
    mix_gain,
    mix_shift,
    gate_in,
    up_in,
    down_out,
    gain,
    shift,
):
    count = lax.axis_size("sp")
    tok_rows, inner = resid.shape
    own = tok_rows // 2
    deep = count // 4
    groups = count // 2
    wide = -(-(gate_in.shape[1] // LANES) // groups)
    span = wide * LANES
    heads = queries.shape[1] // HK
    steps = tok_rows // SPAN
    dma = pltpu.SemaphoreType.DMA
    half, full = jnp.bfloat16, jnp.float32
    block = lambda *lead: pltpu.VMEM((*lead, own, inner), half)
    near, far = pl.BlockSpec(memory_space=pltpu.VMEM), pl.BlockSpec(memory_space=pl.ANY)
    out = pl.pallas_call(
        functools.partial(layer_kernel, deep, wide),
        out_shape=pltpu.VMEM((2, own, inner), half),
        in_specs=[far] * 5 + [near] + [far] * 2 + [near] * 2 + [far] * 3 + [near] * 2,
        out_specs=near,
        scratch_shapes=[
            pltpu.VMEM(queries.shape, half),
            pltpu.VMEM(keys.shape, half),
            pltpu.VMEM(values.shape, half),
            pltpu.VMEM(decay_pre.shape, full),
            pltpu.VMEM(out_gate.shape, half),
            block(2),
            pltpu.VMEM((2, inner, 2 * span), half),
            pltpu.VMEM((2 * span, inner), half),
            pltpu.VMEM(out_proj.shape, half),
            pltpu.VMEM((steps, heads, HK, HV), full),
            pltpu.VMEM((steps, heads, HK, HK), full),
            pltpu.VMEM((heads, HK, HV), half),
            pltpu.VMEM((heads, 8, HK), full),
            pltpu.VMEM((4, HK, HV), half),
            pltpu.VMEM((4, 8, HK), full),
            pltpu.VMEM((4, HK, HV), full),
            pltpu.VMEM((HK, HV), full),
            pltpu.VMEM((HK, HV), half),
            pltpu.VMEM((HK, HV), half),
            pltpu.VMEM((4, HK, HV), half),
            pltpu.VMEM((4, HK, HV), half),
            pltpu.VMEM((tok_rows, out_proj.shape[0]), half),
            block(2),
            block(),
            block(2, deep),
            pltpu.VMEM((2, deep * own, 2 * span), half),
            block(2, deep),
            block(deep),
            block(deep),
            block(deep),
            block(deep - 1),
            pltpu.VMEM((own, inner), full),
            dma((4,)),
            dma((3, groups)),
            dma((3, groups)),
            dma((3, groups)),
            dma((3, groups)),
            dma((2, 2, groups)),
            dma((2, 2, groups)),
            dma((4, 2)),
            dma((4, 2)),
            dma((2,)),
            dma((4,)),
            dma((4,)),
            dma((2,)),
            *[dma((deep, 2))] * 5,
            *[dma((deep, 4))] * 5,
            dma((2, 2)),
            pltpu.SemaphoreType.REGULAR,
            dma((6,)),
        ],
        compiler_params=pltpu.CompilerParams(
            collective_id=2, has_side_effects=True, vmem_limit_bytes=60 * 1024 * 1024
        ),
    )(
        queries,
        keys,
        values,
        decay_pre,
        out_gate,
        head_gain[None],
        out_proj,
        resid.reshape(2, own, inner),
        mix_gain[None],
        mix_shift[None],
        gate_in,
        up_in,
        down_out,
        gain[None],
        shift[None],
    )
    return out.reshape(tok_rows, inner)


def body(
    resid,
    queries,
    keys,
    values,
    decay_pre,
    out_gate,
    head_gain,
    out_proj,
    mix_gain,
    mix_shift,
    gate_in,
    up_in,
    down_out,
    out_gain,
    out_shift,
):
    tp_count = lax.axis_size("tp")
    tok_rows = queries.shape[0]
    own_count = tok_rows // tp_count
    sp_count = lax.axis_size("sp")
    units = gate_in.shape[1]
    heads = queries.shape[1] // HK
    groups = sp_count // 2
    unit_blocks = units // LANES
    by_units = (
        tp_count == 2
        and sp_count == 16
        and heads == 4
        and units % LANES == 0
        and unit_blocks % groups == groups - 2
        and gate_in.shape[0] % LANES == 0
        and down_out.shape[1] % LANES == 0
        and gate_in.shape[0] * sp_count == resid.shape[1]
        and own_count % 16 == 0
        and tok_rows % SPAN == 0
    )
    if by_units:
        return layer(
            resid,
            queries,
            keys,
            values,
            decay_pre,
            out_gate,
            head_gain,
            out_proj,
            mix_gain,
            mix_shift,
            gate_in,
            up_in,
            down_out,
            out_gain,
            out_shift,
        )
    local = local_tokens(queries, keys, values, decay_pre)
    gated = mix_tokens(*local, out_gate, head_gain)
    mixed = lax.psum_scatter(
        jnp.dot(gated, out_proj, preferred_element_type=jnp.float32).astype(jnp.bfloat16),
        "tp",
        scatter_dimension=0,
        tiled=True,
    ).astype(jnp.float32)
    own_resid = lax.dynamic_slice_in_dim(resid, lax.axis_index("tp") * own_count, own_count, 0)
    mid = layer_norm(ALPHA * own_resid.astype(jnp.float32) + mixed, mix_gain, mix_shift).astype(
        jnp.bfloat16
    )
    whole_rows = lax.all_gather(mid, "tp", axis=0, tiled=True)
    hidden = hidden_by_rows(whole_rows, gate_in, up_in)
    ffn = lax.psum_scatter(
        down_by_columns(hidden, down_out).astype(jnp.bfloat16),
        "tp",
        scatter_dimension=0,
        tiled=True,
    ).astype(jnp.float32)
    finished = layer_norm(ALPHA * mid.astype(jnp.float32) + 0.5 * ffn, out_gain, out_shift).astype(
        jnp.bfloat16
    )
    return lax.all_gather(finished, "tp", axis=0, tiled=True)


def solution(mesh):
    return jax.shard_map(
        body,
        mesh=mesh,
        in_specs=(
            P("sp", None),
            P("sp", "tp"),
            P("sp", "tp"),
            P("sp", "tp"),
            P("sp", "tp"),
            P("sp", "tp"),
            P(),
            P("tp", None),
            P(),
            P(),
            P("sp", "tp"),
            P("sp", "tp"),
            P("tp", "sp"),
            P(),
            P(),
        ),
        out_specs=P("sp", None),
        check_vma=False,
    )
```

```python
import functools

import jax
import jax.numpy as jnp
from jax import lax
from jax.experimental import pallas as pl
from jax.experimental.pallas import tpu as pltpu
from jax.sharding import PartitionSpec as P

HK = 128
HV = 256
SPAN = 64
LANES = 128


ALPHA = 2.0**0.25
LN_EPS = 1e-05
RMS_EPS = 1e-06
TAU = 16.0
MESH = pl.DeviceIdType.MESH


def entering(array, axis, combine, identity):
    count, place = (lax.axis_size(axis), lax.axis_index(axis))
    everything = jax.tree.map(
        lambda part, kind: lax.all_gather(part.astype(kind), axis),
        array,
        (jnp.bfloat16, jnp.bfloat16),
    )
    start = jax.tree.map(
        lambda part, zero: jnp.broadcast_to(jnp.asarray(zero, part.dtype), part.shape),
        array,
        identity,
    )

    def lap(k, before):
        reached = k < place
        new = combine(
            before, jax.tree.map(lambda part, own: part[k].astype(own.dtype), everything, array)
        )
        return jax.tree.map(lambda a, b: jnp.where(reached, a, b), new, before)

    return lax.fori_loop(0, count, lap, start)


def layer_norm(inputs, gain, shift):
    center = inputs - jnp.mean(inputs, axis=-1, keepdims=True)
    spread = jnp.mean(center * center, axis=-1, keepdims=True)
    return center * lax.rsqrt(spread + LN_EPS) * gain + shift


def combine_states(earlier, later):
    return (earlier[0] * later[0], later[0][..., None] * earlier[1] + later[1])


def greet(places):
    barrier = pltpu.get_barrier_semaphore()
    for place in places:
        pl.semaphore_signal(barrier, inc=1, device_id=place, device_id_type=MESH)
    pl.semaphore_wait(barrier, len(places))


def remote(src, dst, send, recv, place):
    return pltpu.make_async_remote_copy(
        src_ref=src, dst_ref=dst, send_sem=send, recv_sem=recv, device_id=place, device_id_type=MESH
    )


def local_tokens(queries, keys, values, decay_pre):
    tok_rows = queries.shape[0]
    local_heads = queries.shape[1] // HK
    blocks = tok_rows // SPAN
    logdecay = jax.nn.log_sigmoid(decay_pre) / TAU
    scaled_q = queries.astype(jnp.float32).reshape(blocks, SPAN, local_heads, HK) * HK ** (-0.5)
    key_block = keys.astype(jnp.float32).reshape(blocks, SPAN, local_heads, HK)
    value_block = values.astype(jnp.float32).reshape(blocks, SPAN, local_heads, HV)
    cumul = jnp.cumsum(logdecay.reshape(blocks, SPAN, local_heads, HK), axis=1)
    last = cumul[:, -1]
    key_decayed = key_block * jnp.exp(last[:, None] - cumul)
    updates = jnp.einsum(
        "nchk,nchv->nhkv", key_decayed, value_block, precision=lax.Precision.HIGHEST
    )

    def advance(running_state, inputs):
        decay_end, state_increment, current_query = inputs
        running_state = jnp.exp(decay_end)[..., None] * running_state + state_increment
        return (
            running_state,
            jnp.einsum(
                "qpy,pyr->qpr", current_query, running_state, precision=lax.Precision.HIGHEST
            ),
        )

    own_state, local_read = lax.scan(
        advance, jnp.zeros((local_heads, HK, HV), jnp.float32), (last, updates, scaled_q)
    )
    block_ends = jnp.cumsum(last, axis=0)
    own_decay = jnp.exp(block_ends[-1])
    carry_q = scaled_q * jnp.exp(block_ends)[:, None]
    return local_read, carry_q, own_decay, own_state


def mix_tokens(local_read, carry_q, own_decay, own_state, out_gate, head_gain):
    blocks, span, local_heads, _ = carry_q.shape
    tok_rows = blocks * span
    identity = (jnp.ones_like(own_decay), jnp.zeros_like(own_state))
    _, incoming = entering((own_decay, own_state), "sp", combine_states, identity)
    carried = jnp.einsum(
        "xepj,pjw->xepw", carry_q, incoming, precision=lax.Precision.HIGHEST
    )
    state_readout = (local_read + carried).reshape(tok_rows, local_heads, HV)
    normed = (
        state_readout
        * lax.rsqrt(jnp.mean(state_readout * state_readout, axis=-1, keepdims=True) + RMS_EPS)
        * head_gain
    )
    return (
        normed.reshape(tok_rows, local_heads * HV) * jax.nn.silu(out_gate.astype(jnp.float32))
    ).astype(jnp.bfloat16)


def hidden_by_rows(whole_rows, gate_in, up_in):
    gate = jnp.dot(
        whole_rows,
        lax.all_gather(gate_in, "sp", axis=0, tiled=True),
        preferred_element_type=jnp.float32,
    )
    upward = jnp.dot(
        whole_rows,
        lax.all_gather(up_in, "sp", axis=0, tiled=True),
        preferred_element_type=jnp.float32,
    )
    return (jax.nn.silu(gate) * upward).astype(jnp.bfloat16)


def down_by_columns(hidden, down_out):
    return jnp.dot(
        hidden,
        lax.all_gather(down_out, "sp", axis=1, tiled=True),
        preferred_element_type=jnp.float32,
    )


def layer_kernel(
    deep,
    wide,
    queries_far,
    keys_far,
    values_far,
    decay_pre_far,
    out_gate_far,
    head_gain,
    out_proj,
    resid_far,
    mix_gain,
    mix_shift,
    gate_in,
    up_in,
    down_out,
    gain,
    shift,
    out,
    queries,
    keys,
    values,
    decay_pre,
    out_gate,
    resid,
    w1,
    w2,
    proj,
    updates,
    ends,
    s_out,
    d_out,
    s_in,
    d_in,
    before,
    total,
    t_out,
    t_in,
    s_start,
    start,
    gated,
    mixed,
    mixed_in,
    rows,
    hidden,
    part,
    y_in,
    u_in,
    v_in,
    z_out,
    acc,
    own_sem,
    b_send,
    b_recv,
    f_send,
    f_recv,
    t_send,
    t_recv,
    p1_send,
    p1_recv,
    p2_sem,
    p3_send,
    p3_recv,
    m_sem,
    au_send,
    av_send,
    ay_send,
    az_recv,
    ay_recv,
    ry_send,
    ry_recv,
    rz_send,
    ru_recv,
    rv_recv,
    f_sem,
    go_sem,
    near_sem,
):
    me, core = lax.axis_index("sp"), lax.axis_index("tp")
    x, y, z = me % 2, (me // 2) % 2, me // 4
    group = me // 2
    groups = 2 * deep
    plane = 4
    place = me % plane
    own, inner = rows.shape[2], rows.shape[3]
    depth = gate_in.shape[0]
    lanes = down_out.shape[1]
    span = wide * LANES
    half = lambda c: pl.ds(pl.multiple_of(c * span, span), span)
    twin = (me, 1 - core)
    x_place = (me + 1 - 2 * x, core)
    y_place = (me + 2 - 4 * y, core)
    above, below = (me + plane, core), (me - plane, core)
    sides = [(dy, dz) for dz in range(deep) for dy in range(2)]
    bottom = z < deep // 2
    edge = jnp.logical_or(z == 0, z == deep - 1)
    pair = z + 1 - 2 * (z % 2)
    inner_z = jnp.where(bottom, deep // 2, deep // 2 - 1)
    edge_z = jnp.where(bottom, deep - 1, 0)

    def at(xx, yy, zz):
        return (plane * zz + 2 * yy + xx, core)

    def target(dy, dz):
        return (y + dy) % 2, (z + dz) % deep

    def origin(dy, dz):
        return (y + dy) % 2, (z + deep - dz) % deep

    def fellow(dp):
        return (x + dp % 2) % 2, (y + dp // 2) % 2

    def short(c, g):
        return jnp.logical_or(g == c, g == groups - 2 + c)

    def first_block(c, g):
        return wide * g - (g > c).astype(jnp.int32) - (g > groups - 2 + c).astype(jnp.int32)

    def sized(flag, run):
        @pl.when(flag)
        def _():
            run(wide - 1)

        @pl.when(jnp.logical_not(flag))
        def _():
            run(wide)

    def taken(mat, g, blocks):
        begin = pl.ds(pl.multiple_of(first_block(core, g) * LANES, LANES), blocks * LANES)
        return (gate_in.at[:, begin], up_in.at[:, begin], down_out.at[begin])[mat]

    def landing(mat, c, s, blocks):
        if mat < 2:
            rows_of = pl.ds(pl.multiple_of(s * depth, depth), depth)
            return w1.at[c, rows_of, pl.ds(mat * span, blocks * LANES)]
        columns = pl.ds(pl.multiple_of(s * lanes, lanes), lanes)
        return w2.at[pl.ds(pl.multiple_of(c * span, span), blocks * LANES), columns]

    def slab(j, c, s):
        if j == 0:
            return w1.at[c, pl.ds(pl.multiple_of(s * depth, depth), depth)]
        return landing(2, c, s, wide)

    def home(dy, dz):
        return isinstance(dz, int) and dy == 0 and dz == 0

    def bring(mat, dy, dz, run):
        yy, zz = target(dy, dz)
        goal = x_place if home(dy, dz) else at(x, yy, zz)
        g = 2 * zz + yy
        r = 2 * dz + dy

        def copy(blocks):
            run(
                remote(
                    taken(mat, g, blocks),
                    landing(mat, core, me, blocks),
                    b_send.at[mat, r],
                    b_recv.at[mat, r],
                    goal,
                )
            )

        sized(short(core, g), copy)

    def send(mat, dy, dz):
        bring(mat, dy, dz, lambda copy: copy.start())

    def send_near(mat):
        send(mat, 0, 0)
        send(mat, 1, 0)

    def send_to(mat, dy, zz):
        send(mat, dy, (zz + deep - z) % deep)

    def source(dy, dz, k):
        yy, zz = origin(dy, dz)
        return plane * zz + 2 * yy + (x + k) % 2

    def relay(mat, dy, dz, run):
        r = 2 * dz + dy

        def copy(blocks):
            block = landing(mat, core, source(dy, dz, 0), blocks)
            run(remote(block, block, f_send.at[mat, r], f_recv.at[mat, r], x_place))

        sized(short(core, group), copy)

    def share(j, k, dy, dz):
        block = slab(j, core, source(dy, dz, k))
        r = 2 * dz + dy
        return remote(block, block, t_send.at[j, k, r], t_recv.at[j, k, r], twin)

    def came(ref, sem):
        remote(ref, ref, f_sem.at[0, 0], sem, twin).wait_recv()

    def shared(mat, k, dy, dz):
        if mat:
            share(mat - 1, k, dy, dz).start()

    def pass_on(mat, dy, dz):
        k = 1 if home(dy, dz) else 0
        sized(
            short(core, group),
            lambda blocks: came(
                landing(mat, core, source(dy, dz, k), blocks), b_recv.at[mat, 2 * dz + dy]
            ),
        )
        if not k:
            relay(mat, dy, dz, lambda copy: copy.start())
        shared(mat, k, dy, dz)

    def pass_on_near(mat):
        pass_on(mat, 0, 0)
        pass_on(mat, 1, 0)

    def pass_on_from(mat, dy, zz):
        pass_on(mat, dy, (z + deep - zz) % deep)

    def passed(mat, *levels):
        def one(dy, dz):
            sized(
                short(core, group),
                lambda blocks: came(
                    landing(mat, core, source(dy, dz, 1), blocks), f_recv.at[mat, 2 * dz + dy]
                ),
            )
            shared(mat, 1, dy, dz)

        for zz in levels:
            if zz is None:
                one(1, 0)
            else:
                for dy in range(2):
                    one(dy, (z + deep - zz) % deep)

    def local(mat, run):
        def copy(blocks):
            run(
                pltpu.make_async_copy(
                    taken(mat, group, blocks), landing(mat, core, me, blocks), own_sem.at[mat]
                )
            )

        sized(short(core, group), copy)

    keep_proj = pltpu.make_async_copy(out_proj, proj, own_sem.at[3])

    keep_near = [
        pltpu.make_async_copy(ref, copy, near_sem.at[i])
        for i, (ref, copy) in enumerate(
            (
                (decay_pre_far, decay_pre),
                (keys_far, keys),
                (values_far, values),
                (queries_far, queries),
                (out_gate_far, out_gate),
                (resid_far, resid),
            )
        )
    ]
    for copy in keep_near:
        copy.start()

    with jax.named_scope("greet"):
        partners = [at(x, *target(dy, dz)) for dy, dz in sides[1:]]
        partners += [x_place, at(*fellow(3), z), twin]
        greet(partners)
    for zz in (inner_z, edge_z, pair):
        send_to(0, 0, zz)
    for mat in range(3):
        local(mat, lambda copy: copy.start())
    keep_proj.start()

    with jax.named_scope("local"):
        for copy in keep_near[:3]:
            copy.wait()
        tokens = queries.shape[0]
        heads = queries.shape[1] // HK
        blocks = tokens // SPAN
        raw = decay_pre[...]
        logdecay = (jnp.minimum(raw, 0.0) - jnp.log1p(jnp.exp(-jnp.abs(raw)))) / TAU
        row = lax.broadcasted_iota(jnp.int32, (tokens, tokens), 0)
        col = lax.broadcasted_iota(jnp.int32, (tokens, tokens), 1)
        tri = jnp.logical_and(row // SPAN == col // SPAN, col <= row).astype(jnp.float32)
        cumul = jnp.dot(
            tri, logdecay, precision=lax.Precision.HIGHEST, preferred_element_type=jnp.float32
        )
        lasts = [cumul[(n + 1) * SPAN - 1 : (n + 1) * SPAN] for n in range(blocks)]
        across = (((0,), (0,)), ((), ()))

        def column(line):
            return jnp.broadcast_to(line, (HK, HK)).T

        def spread(square):
            return jnp.concatenate([square] * (HV // HK), axis=1)

        for n in range(blocks):
            steps = slice(n * SPAN, (n + 1) * SPAN)
            faded = keys[steps].astype(jnp.float32) * jnp.exp(lasts[n] - cumul[steps])
            high = faded.astype(jnp.bfloat16)
            low = (faded - high.astype(jnp.float32)).astype(jnp.bfloat16)
            for h in range(heads):
                key = slice(h * HK, (h + 1) * HK)
                value = values[steps, h * HV : (h + 1) * HV]
                updates[n, h] = lax.dot_general(
                    high[:, key], value, across, preferred_element_type=jnp.float32
                ) + lax.dot_general(
                    low[:, key], value, across, preferred_element_type=jnp.float32
                )
                ends[n, h] = column(jnp.exp(lasts[n][:, key]))
        whole = jnp.exp(sum(lasts))
        for h in range(heads):
            state = updates[0, h]
            for n in range(1, blocks):
                state = spread(ends[n, h]) * state + updates[n, h]
            s_out[h] = state.astype(jnp.bfloat16)
            d_out[h] = jnp.broadcast_to(whole[:, h * HK : (h + 1) * HK], d_out.shape[1:])

    def to_plane(dp):
        xx, yy = fellow(dp)
        goal, slot = at(xx, yy, z), 2 * yy + xx
        return (
            remote(s_out.at[slot], s_in.at[place], p1_send.at[dp, 0], p1_recv.at[dp, 0], goal),
            remote(d_out.at[slot], d_in.at[place], p1_send.at[dp, 1], p1_recv.at[dp, 1], goal),
        )

    for dp in range(1, plane):
        for copy in to_plane(dp):
            copy.start()
    s_in[place] = s_out[place]
    d_in[place] = d_out[place]
    send_near(0)

    @pl.when(short(core, group))
    def _():
        last_block = (wide - 1) * LANES
        blank = jnp.zeros((w1.shape[1], LANES), jnp.bfloat16)
        w1[core, :, last_block:span] = blank
        w1[core, :, span + last_block :] = blank
        tail = pl.ds(pl.multiple_of(core * span + last_block, LANES), LANES)
        w2[tail] = jnp.zeros((LANES, inner), jnp.bfloat16)

    with jax.named_scope("p1"):
        for dp in range(1, plane):
            for copy in to_plane(dp):
                copy.wait_recv()
    running = jnp.zeros((HK, HV), jnp.float32)
    line = jnp.ones((1, HK), jnp.float32)
    reach = []
    for i in range(plane):
        before[i] = running
        reach.append(line)
        own_decay = d_in[i][:1]
        running = spread(column(own_decay)) * running + s_in[i].astype(jnp.float32)
        line = line * own_decay
    total[...] = jnp.zeros(total.shape, jnp.float32)

    def to_next():
        return remote(t_out, t_in, p2_sem.at[0], p2_sem.at[1], above)

    def push_on():
        t_out[...] = (spread(column(line)) * total[...] + running).astype(jnp.bfloat16)
        to_next().start()

    @pl.when(z == 0)
    def _():
        push_on()

    @pl.when(jnp.logical_not(bottom))
    def _():
        for mat, dy, zz in ((1, 0, inner_z), (1, 0, edge_z), (0, 1, inner_z)):
            send_to(mat, dy, zz)

    def gates():
        pass_on_near(0)
        for zz in (pair, edge_z, inner_z):
            pass_on_from(0, 0, zz)

    with jax.named_scope("gates1"):

        @pl.when(jnp.logical_not(bottom))
        def _():
            gates()

    with jax.named_scope("p2"):

        @pl.when(z > 0)
        def _():
            came(t_in, p2_sem.at[1])
            total[...] = t_in[...].astype(jnp.float32)

    @pl.when(jnp.logical_and(z > 0, z < deep - 1))
    def _():
        push_on()

    for i in range(plane):
        s_start[i] = (before[i] + spread(column(reach[i])) * total[...]).astype(jnp.bfloat16)

    def to_fellow(dp):
        xx, yy = fellow(dp)
        slot = 2 * yy + xx
        return remote(
            s_start.at[slot], start.at[place], p3_send.at[dp], p3_recv.at[dp], at(xx, yy, z)
        )

    for dp in range(1, plane):
        to_fellow(dp).start()
    start[place] = s_start[place]
    send_to(1, 0, pair)
    send_to(2, 0, pair)
    send_to(0, 1, pair)

    @pl.when(bottom)
    def _():
        for zz in (inner_z, edge_z):
            send_to(1, 0, zz)
            send_to(0, 1, zz)

    @pl.when(jnp.logical_not(bottom))
    def _():
        send_to(0, 1, edge_z)

    send_near(1)
    send_near(2)
    with jax.named_scope("gates2"):

        @pl.when(bottom)
        def _():
            gates()

    with jax.named_scope("p3"):
        for dp in range(1, plane):
            to_fellow(dp).wait_recv()

    with jax.named_scope("mix"):
        for copy in keep_near[3:]:
            copy.wait()
        for h in range(heads):
            thick = slice(h * HV, (h + 1) * HV)
            state = start[h].astype(jnp.float32)
            reads = []
            for n in range(blocks):
                state = spread(ends[n, h]) * state + updates[n, h]
                high = state.astype(jnp.bfloat16)
                low = (state - high.astype(jnp.float32)).astype(jnp.bfloat16)
                query = queries[n * SPAN : (n + 1) * SPAN, h * HK : (h + 1) * HK]
                reads.append(
                    jnp.dot(query, high, preferred_element_type=jnp.float32)
                    + jnp.dot(query, low, preferred_element_type=jnp.float32)
                )
            read = jnp.concatenate(reads, axis=0) * HK ** (-0.5)
            size = jnp.mean(read * read, axis=-1, keepdims=True)
            pre = out_gate[:, thick].astype(jnp.float32)
            normed = read * lax.rsqrt(size + RMS_EPS) * head_gain[...]
            gated[:, thick] = (normed * (pre * jax.nn.sigmoid(pre))).astype(jnp.bfloat16)
    keep_proj.wait()
    with jax.named_scope("proj"):
        summed_heads = jnp.dot(gated[...], proj[...], preferred_element_type=jnp.float32)
        mixed[...] = summed_heads.astype(jnp.bfloat16).reshape(2, own, inner)
    swap = remote(mixed.at[1 - core], mixed_in, m_sem.at[0], m_sem.at[1], twin)
    swap.start()
    with jax.named_scope("swap"):
        swap.wait()
    with jax.named_scope("ln"):
        added = mixed[core].astype(jnp.float32) + mixed_in[...].astype(jnp.float32)
        middle = ALPHA * resid[core].astype(jnp.float32) + added
        rows[y, z] = layer_norm(middle, mix_gain[...], mix_shift[...]).astype(jnp.bfloat16)

    halves = range(2)
    chunk = own // 2
    bit = [pl.ds(h * chunk, chunk) for h in halves]

    def climb(zz, h):
        block = rows.at[y, zz, bit[h]]
        return remote(block, block, au_send.at[zz, h], az_recv.at[zz, h], above)

    def sink(zz, h):
        block = rows.at[y, zz, bit[h]]
        return remote(block, block, av_send.at[zz, h], az_recv.at[zz, h], below)

    def cross_y(zz, h):
        block = rows.at[y, zz, bit[h]]
        return remote(block, block, ay_send.at[zz, h], ay_recv.at[zz, h], y_place)

    for h in halves:

        @pl.when(z < deep - 1)
        def _():
            climb(z, h).start()

        @pl.when(z > 0)
        def _():
            sink(z, h).start()

        cross_y(z, h).start()

    ahead = jnp.logical_not(jnp.logical_or(bottom, edge))

    @pl.when(ahead)
    def _():
        for zz in (inner_z, edge_z):
            send_to(1, 1, zz)

    def landed(far):
        for h in halves:

            @pl.when(z >= far)
            def _():
                came(rows.at[y, z - far, bit[h]], az_recv.at[z - far, h])

                @pl.when(z < deep - 1)
                def _():
                    climb(z - far, h).start()

                cross_y(z - far, h).start()

            @pl.when(z < deep - far)
            def _():
                came(rows.at[y, z + far, bit[h]], az_recv.at[z + far, h])

                @pl.when(z > 0)
                def _():
                    sink(z + far, h).start()

                cross_y(z + far, h).start()

    with jax.named_scope("wa"):
        for mat in range(3):
            local(mat, lambda copy: copy.wait())
        share(0, 0, 0, 0).start()
        share(1, 0, 0, 0).start()
        pass_on_near(1)
        for zz in (pair, edge_z, inner_z):
            pass_on_from(1, 0, zz)
        pass_on_from(0, 1, pair)
        pass_on_from(2, 0, pair)
    with jax.named_scope("ag1"):
        landed(1)

    send_to(1, 1, pair)
    send_to(2, 1, pair)

    def second_wave():
        @pl.when(jnp.logical_not(ahead))
        def _():
            for zz in (inner_z, edge_z):
                send_to(1, 1, zz)

        for dy in range(2):
            for zz in (inner_z, edge_z):
                send_to(2, dy, zz)

    @pl.when(jnp.logical_not(edge))
    def _():
        second_wave()

    with jax.named_scope("wb"):
        for zz in (edge_z, inner_z):
            pass_on_from(0, 1, zz)
        pass_on_near(2)
    with jax.named_scope("ag2"):
        landed(2)

    @pl.when(jnp.logical_not(edge))
    def _():
        pl.semaphore_signal(
            go_sem, inc=1, device_id=at(x, y, edge_z), device_id_type=MESH
        )

    with jax.named_scope("wc"):
        pass_on_from(1, 1, pair)
        pass_on_from(2, 1, pair)

    with jax.named_scope("go"):

        @pl.when(edge)
        def _():
            pl.semaphore_wait(go_sem, 1)
            second_wave()

    with jax.named_scope("ag3"):
        for far in range(3, deep):
            landed(far)
    with jax.named_scope("wd0"):
        passed(0, None, pair, edge_z, inner_z)
        passed(1, None, pair)
    with jax.named_scope("wd"):
        pass_on_from(1, 1, inner_z)
        pass_on_from(1, 1, edge_z)
        passed(2, None, pair)
        pass_on_from(2, 0, edge_z)
        pass_on_from(2, 0, inner_z)
    def last_blocks():
        pass_on_from(2, 1, edge_z)
        pass_on_from(2, 1, inner_z)

    with jax.named_scope("we"):

        @pl.when(jnp.logical_not(bottom))
        def _():
            last_blocks()

    with jax.named_scope("wf"):
        passed(1, edge_z, inner_z)
    with jax.named_scope("agy"):
        for zz in range(deep):
            for h in halves:
                came(rows.at[1 - y, zz, bit[h]], ay_recv.at[zz, h])
    def twins(j, *levels):
        for zz in levels:
            dz = 0 if zz is None else (z + deep - zz) % deep
            for k in range(2):
                for dy in range(2):
                    came(slab(j, 1 - core, source(dy, dz, k)), t_recv.at[j, k, 2 * dz + dy])

    with jax.named_scope("wt"):
        twins(0, None, pair, edge_z, inner_z)

    def hide(side, slot):
        left = rows[side].reshape(deep * own, inner)
        for c in range(2):
            both = jnp.dot(left, w1[c], preferred_element_type=jnp.float32)
            gate, up = both[:, :span], both[:, span:]
            hidden[slot, :, c * span : (c + 1) * span] = (
                gate * jax.nn.sigmoid(gate) * up
            ).astype(jnp.bfloat16)

    wing = inner // 2
    early = jnp.where(bottom, 0, 1)
    late = 1 - early
    columns = lambda h: pl.ds(pl.multiple_of(h * wing, wing), wing)

    def lower(side, slot, h):
        down = jnp.dot(hidden[slot], w2[:, columns(h)], preferred_element_type=jnp.float32)
        part[side, :, :, columns(h)] = down.astype(jnp.bfloat16).reshape(deep, own, wing)

    order = [
        jnp.where(bottom, deep - 1, 0),
        jnp.where(bottom, deep - 2, 1),
        jnp.where(bottom, 1 - z, 2 * deep - 3 - z),
        z,
    ]

    slim = wing // 4
    columns_of = lambda q: pl.ds(pl.multiple_of(q * slim, slim), slim)
    pieces = lambda h: [4 * h + i for i in range(4)]

    def across_y(d, h):
        return remote(
            part.at[1 - y, d, :, columns_of(h)],
            y_in.at[d, :, columns_of(h)],
            ry_send.at[d, h],
            ry_recv.at[d, h],
            y_place,
        )

    def hop(i, h, up):
        into, sem = (u_in, ru_recv) if up else (v_in, rv_recv)
        return remote(
            z_out.at[i, :, columns_of(h)],
            into.at[order[i], :, columns_of(h)],
            rz_send.at[i, h],
            sem.at[order[i], h],
            above if up else below,
        )

    def gather_in(d, h, from_below, from_above):
        taken = columns_of(h)
        came(y_in.at[d, :, taken], ry_recv.at[d, h])
        acc[:, taken] = part[y, d, :, taken].astype(jnp.float32) + y_in[d, :, taken].astype(
            jnp.float32
        )

        @pl.when(from_below)
        def _():
            came(u_in.at[d, :, taken], ru_recv.at[d, h])
            acc[:, taken] += u_in[d, :, taken].astype(jnp.float32)

        @pl.when(from_above)
        def _():
            came(v_in.at[d, :, taken], rv_recv.at[d, h])
            acc[:, taken] += v_in[d, :, taken].astype(jnp.float32)

    def step(i, h):
        d = order[i]
        up = d > z
        gather_in(
            d,
            h,
            jnp.logical_and(up, z > 0),
            jnp.logical_and(jnp.logical_not(up), z < deep - 1),
        )
        z_out[i, :, columns_of(h)] = acc[:, columns_of(h)].astype(jnp.bfloat16)

        @pl.when(up)
        def _():
            hop(i, h, True).start()

        @pl.when(jnp.logical_not(up))
        def _():
            hop(i, h, False).start()

    with jax.named_scope("hide0"):
        hide(1 - y, 0)
    with jax.named_scope("wx"):

        @pl.when(bottom)
        def _():
            last_blocks()

    with jax.named_scope("wg"):
        twins(1, None, pair)
    with jax.named_scope("down0"):
        lower(1 - y, 0, early)
    for d in order[:2]:
        for q in pieces(early):
            across_y(d, q).start()
    with jax.named_scope("hide1"):
        hide(y, 1)
    with jax.named_scope("down1"):
        lower(y, 1, early)
    with jax.named_scope("wh"):
        passed(2, edge_z, inner_z)
        twins(1, edge_z, inner_z)
    with jax.named_scope("down2"):
        lower(1 - y, 0, late)
    for d in order[:2]:
        for q in pieces(late):
            across_y(d, q).start()
    for d in order[2:]:
        for h in (early, late):
            for q in pieces(h):
                across_y(d, q).start()
    with jax.named_scope("down3"):
        lower(y, 1, late)
    for i, h in ((0, early), (1, early), (0, late), (1, late), (2, early), (2, late)):
        with jax.named_scope("rs%d%d" % (i, h is late)):
            for q in pieces(h):
                step(i, q)
    with jax.named_scope("rsend0"):
        for q in pieces(early):
            gather_in(z, q, z > 0, z < deep - 1)
    with jax.named_scope("rsend1"):
        for q in pieces(late):
            gather_in(z, q, z > 0, z < deep - 1)
    with jax.named_scope("fin"):
        finished = layer_norm(
            ALPHA * rows[y, z].astype(jnp.float32) + 0.5 * acc[...], gain[...], shift[...]
        )
        out[core] = finished.astype(jnp.bfloat16)
    last = remote(out.at[core], out.at[core], f_sem.at[0, 0], f_sem.at[1, 0], twin)
    last.start()

    with jax.named_scope("drain"):

        @pl.when(z < deep - 1)
        def _():
            to_next().wait_send()

        for dy, dz in sides:
            for mat in range(3):
                bring(mat, dy, dz, lambda copy: copy.wait_send())
                if (dy, dz) != (0, 0):
                    relay(mat, dy, dz, lambda copy: copy.wait_send())
            for j in range(2):
                for k in range(2):
                    share(j, k, dy, dz).wait_send()
        for dp in range(1, plane):
            for copy in (*to_plane(dp), to_fellow(dp)):
                copy.wait_send()
        for zz in range(deep):

            for h in halves:

                @pl.when(jnp.logical_and(zz <= z, z < deep - 1))
                def _():
                    climb(zz, h).wait_send()

                @pl.when(jnp.logical_and(zz >= z, z > 0))
                def _():
                    sink(zz, h).wait_send()

                cross_y(zz, h).wait_send()
        for q in range(8):
            for i in range(deep):
                across_y(i, q).wait_send()
            for i in range(deep - 1):
                hop(i, q, True).wait_send()
        last.wait()


def layer(
    resid,
    queries,
    keys,
    values,
    decay_pre,
    out_gate,
    head_gain,
    out_proj,
    mix_gain,
    mix_shift,
    gate_in,
    up_in,
    down_out,
    gain,
    shift,
):
    count = lax.axis_size("sp")
    tok_rows, inner = resid.shape
    own = tok_rows // 2
    deep = count // 4
    groups = count // 2
    wide = -(-(gate_in.shape[1] // LANES) // groups)
    span = wide * LANES
    heads = queries.shape[1] // HK
    steps = tok_rows // SPAN
    dma = pltpu.SemaphoreType.DMA
    half, full = jnp.bfloat16, jnp.float32
    block = lambda *lead: pltpu.VMEM((*lead, own, inner), half)
    near, far = pl.BlockSpec(memory_space=pltpu.VMEM), pl.BlockSpec(memory_space=pl.ANY)
    out = pl.pallas_call(
        functools.partial(layer_kernel, deep, wide),
        out_shape=pltpu.VMEM((2, own, inner), half),
        in_specs=[far] * 5 + [near] + [far] * 2 + [near] * 2 + [far] * 3 + [near] * 2,
        out_specs=near,
        scratch_shapes=[
            pltpu.VMEM(queries.shape, half),
            pltpu.VMEM(keys.shape, half),
            pltpu.VMEM(values.shape, half),
            pltpu.VMEM(decay_pre.shape, full),
            pltpu.VMEM(out_gate.shape, half),
            block(2),
            pltpu.VMEM((2, inner, 2 * span), half),
            pltpu.VMEM((2 * span, inner), half),
            pltpu.VMEM(out_proj.shape, half),
            pltpu.VMEM((steps, heads, HK, HV), full),
            pltpu.VMEM((steps, heads, HK, HK), full),
            pltpu.VMEM((heads, HK, HV), half),
            pltpu.VMEM((heads, 8, HK), full),
            pltpu.VMEM((4, HK, HV), half),
            pltpu.VMEM((4, 8, HK), full),
            pltpu.VMEM((4, HK, HV), full),
            pltpu.VMEM((HK, HV), full),
            pltpu.VMEM((HK, HV), half),
            pltpu.VMEM((HK, HV), half),
            pltpu.VMEM((4, HK, HV), half),
            pltpu.VMEM((4, HK, HV), half),
            pltpu.VMEM((tok_rows, out_proj.shape[0]), half),
            block(2),
            block(),
            block(2, deep),
            pltpu.VMEM((2, deep * own, 2 * span), half),
            block(2, deep),
            block(deep),
            block(deep),
            block(deep),
            block(deep - 1),
            pltpu.VMEM((own, inner), full),
            dma((4,)),
            dma((3, groups)),
            dma((3, groups)),
            dma((3, groups)),
            dma((3, groups)),
            dma((2, 2, groups)),
            dma((2, 2, groups)),
            dma((4, 2)),
            dma((4, 2)),
            dma((2,)),
            dma((4,)),
            dma((4,)),
            dma((2,)),
            *[dma((deep, 2))] * 5,
            *[dma((deep, 8))] * 5,
            dma((2, 2)),
            pltpu.SemaphoreType.REGULAR,
            dma((6,)),
        ],
        compiler_params=pltpu.CompilerParams(
            collective_id=2, has_side_effects=True, vmem_limit_bytes=60 * 1024 * 1024
        ),
    )(
        queries,
        keys,
        values,
        decay_pre,
        out_gate,
        head_gain[None],
        out_proj,
        resid.reshape(2, own, inner),
        mix_gain[None],
        mix_shift[None],
        gate_in,
        up_in,
        down_out,
        gain[None],
        shift[None],
    )
    return out.reshape(tok_rows, inner)


def body(
    resid,
    queries,
    keys,
    values,
    decay_pre,
    out_gate,
    head_gain,
    out_proj,
    mix_gain,
    mix_shift,
    gate_in,
    up_in,
    down_out,
    out_gain,
    out_shift,
):
    tp_count = lax.axis_size("tp")
    tok_rows = queries.shape[0]
    own_count = tok_rows // tp_count
    sp_count = lax.axis_size("sp")
    units = gate_in.shape[1]
    heads = queries.shape[1] // HK
    groups = sp_count // 2
    unit_blocks = units // LANES
    by_units = (
        tp_count == 2
        and sp_count == 16
        and heads == 4
        and units % LANES == 0
        and unit_blocks % groups == groups - 2
        and gate_in.shape[0] % LANES == 0
        and down_out.shape[1] % LANES == 0
        and gate_in.shape[0] * sp_count == resid.shape[1]
        and own_count % 16 == 0
        and tok_rows % SPAN == 0
    )
    if by_units:
        return layer(
            resid,
            queries,
            keys,
            values,
            decay_pre,
            out_gate,
            head_gain,
            out_proj,
            mix_gain,
            mix_shift,
            gate_in,
            up_in,
            down_out,
            out_gain,
            out_shift,
        )
    local = local_tokens(queries, keys, values, decay_pre)
    gated = mix_tokens(*local, out_gate, head_gain)
    mixed = lax.psum_scatter(
        jnp.dot(gated, out_proj, preferred_element_type=jnp.float32).astype(jnp.bfloat16),
        "tp",
        scatter_dimension=0,
        tiled=True,
    ).astype(jnp.float32)
    own_resid = lax.dynamic_slice_in_dim(resid, lax.axis_index("tp") * own_count, own_count, 0)
    mid = layer_norm(ALPHA * own_resid.astype(jnp.float32) + mixed, mix_gain, mix_shift).astype(
        jnp.bfloat16
    )
    whole_rows = lax.all_gather(mid, "tp", axis=0, tiled=True)
    hidden = hidden_by_rows(whole_rows, gate_in, up_in)
    ffn = lax.psum_scatter(
        down_by_columns(hidden, down_out).astype(jnp.bfloat16),
        "tp",
        scatter_dimension=0,
        tiled=True,
    ).astype(jnp.float32)
    finished = layer_norm(ALPHA * mid.astype(jnp.float32) + 0.5 * ffn, out_gain, out_shift).astype(
        jnp.bfloat16
    )
    return lax.all_gather(finished, "tp", axis=0, tiled=True)


def solution(mesh):
    return jax.shard_map(
        body,
        mesh=mesh,
        in_specs=(
            P("sp", None),
            P("sp", "tp"),
            P("sp", "tp"),
            P("sp", "tp"),
            P("sp", "tp"),
            P("sp", "tp"),
            P(),
            P("tp", None),
            P(),
            P(),
            P("sp", "tp"),
            P("sp", "tp"),
            P("tp", "sp"),
            P(),
            P(),
        ),
        out_specs=P("sp", None),
        check_vma=False,
    )
```
